128 devices in a mesh: sp: 16 (over z, y), tp: 8 (over x, core).
Axes of the slice: x: 4, y: 4, z: 4, core: 2. Of those that a mesh axis runs over, the one named last changes fastest.
Arguments:
- tokens: bfloat16 [16384, 2048], P('sp'), may hold values from -6 to 6
- norm_gain: float32 [2048], replicated, may hold values from 0.1 to 1.9
- attn_query: bfloat16 [2048, 1024], P(None, 'tp'), may hold values from -0.088388348 to 0.088388348
- attn_key: bfloat16 [2048, 1024], P(None, 'tp'), may hold values from -0.088388348 to 0.088388348
- attn_value: bfloat16 [2048, 1024], P(None, 'tp'), may hold values from -0.125 to 0.125
- score_scale: float32 [16], replicated, may hold values from 0.5 to 40
- attention_decay: float32 [16, 16384], P('tp'), as said below
- mem_query: bfloat16 [2048, 1024], P(None, 'tp'), may hold values from -0.125 to 0.125
- mem_key: bfloat16 [2048, 1024], P(None, 'tp'), may hold values from -0.125 to 0.125
- mem_value: bfloat16 [2048, 1024], P(None, 'tp'), may hold values from -0.125 to 0.125
- mem_ingate: bfloat16 [2048, 8], replicated, may hold values from -0.125 to 0.125
- input_shift: float32 [8], replicated, may hold values from -3 to 100
- memory_decay: float32 [8, 16384], P('tp', 'sp'), may hold values from -1.5 to 0
- mem_outgate: bfloat16 [2048, 1024], P(None, 'tp'), may hold values from -0.125 to 0.125
- init_memory: float32 [8, 128, 128], P('tp'), may hold values from -192 to 192
- init_normalizer: float32 [8, 128], P('tp'), may hold values from -192 to 192
- attn_gain: float32 [1024], replicated, may hold values from 0.1 to 1.9
- mem_gain: float32 [1024], replicated, may hold values from 0.1 to 1.9
- attn_out: bfloat16 [1024, 2048], replicated, may hold values from -0.125 to 0.125
- mem_out: bfloat16 [1024, 2048], replicated, may hold values from -0.125 to 0.125
Outputs:
- mixed: bfloat16 [16384, 2048], P(('sp', 'tp'))
The draws below stay inside these ranges and needn't reach their ends.
Inputs may be any that keep to these rules, and one draw needn't show every extreme that they name: `attention_decay`: each head's row never rises from one position to the next.
All inputs are finite; a program needn't handle non-finite values.
Results may differ from the reference program's by a relative error of at most 0.025.
The reference program's roundings to bfloat16 on the way (of `normed`, `att_mix` and `mem_mix`) count: a program that leaves them out, or rounds other values in their place, can miss the bound.
Values may be sent and summed in bfloat16 or wider, within the bound.
A program may use at most 128 MiB of HBM per device.

```python
import math
import jax
import jax.numpy as jnp
from jax import lax

D = 2048
AHEADS = 16
ADIM = 64
MHEADS = 8
MDIM = 128
BLOCK = 128
TOK_DEV = 1024
SEQUENCE_LENGTH = 16384
N_SP = 16


def loguniform_draw(key, shape, lower, upper):
    return jnp.exp(jax.random.uniform(key, shape, jnp.float32, math.log(lower), math.log(upper)))


def paired_channels(key):
    order = jax.random.permutation(jax.random.fold_in(key, 31), jnp.arange(D, dtype=jnp.int32))
    swapped = order.reshape(D // 2, 2)[:, ::-1].reshape(D)
    return jnp.zeros((D,), jnp.int32).at[order].set(swapped)


def query_matrix(key):
    raw = jax.random.normal(jax.random.fold_in(key, 32), (D, AHEADS * ADIM), jnp.float32)
    return jnp.clip(raw, -4.0, 4.0) * D ** (-0.5)


def draw_attn_query(key, part):
    return query_matrix(key).astype(jnp.bfloat16)


def draw_attn_key(key, part):
    partner = paired_channels(key)
    return query_matrix(key)[partner].astype(jnp.bfloat16)


def draw_norm_gain(key, part):
    partner = paired_channels(key)
    raw = jax.random.normal(jax.random.fold_in(key, 33), (D,), jnp.float32)
    pair_gain = jnp.clip(1.0 + 0.18 * raw, 0.1, 1.9)
    lower_index = jnp.minimum(jnp.arange(D, dtype=jnp.int32), partner)
    return pair_gain[lower_index]


def draw_tokens(key, part):
    partner = paired_channels(key)
    base = jnp.clip(jax.random.normal(jax.random.fold_in(key, 34), (SEQUENCE_LENGTH, D), jnp.float32), -6.0, 6.0)
    plant_count = SEQUENCE_LENGTH // 32
    offsets = jax.random.randint(jax.random.fold_in(key, 35), (plant_count,), 0, 32)
    targets = (32 * jnp.arange(plant_count, dtype=jnp.int32) + offsets).astype(jnp.int32)
    exponents = jax.random.uniform(jax.random.fold_in(key, 36), (plant_count,), jnp.float32, 0.25, 1.0)
    reach = jnp.floor(jnp.exp(exponents * jnp.log(jnp.maximum(targets, 2).astype(jnp.float32)))).astype(jnp.int32)
    reach = jnp.clip(reach, 1, jnp.maximum(targets, 1))
    sources = jnp.maximum(targets - reach, 0).astype(jnp.int32)

    def plant(index, rows):
        target = targets[index]
        copied = rows[sources[index]][partner]
        chosen = jnp.where(target >= 8, copied, rows[target])
        return rows.at[target].set(chosen)
    planted = lax.fori_loop(0, plant_count, plant, base)
    return planted.astype(jnp.bfloat16)


def decay_steps(key, number_of_heads):
    random_subkeys = jax.random.split(key, 7)
    slow_share = 0.5
    slow_head = jax.random.uniform(random_subkeys[0], (number_of_heads, 1), jnp.float32) < slow_share
    slow_rate = loguniform_draw(random_subkeys[1], (number_of_heads, 1), 0.2, 0.4) / SEQUENCE_LENGTH
    fast_rate = loguniform_draw(random_subkeys[2], (number_of_heads, 1), 0.01, 1.0 / 30.0)
    learning_rate = jnp.where(slow_head, slow_rate, fast_rate)
    block_multiplier = jnp.repeat(loguniform_draw(random_subkeys[3], (number_of_heads, SEQUENCE_LENGTH // TOK_DEV), 0.5, 2.0), TOK_DEV, axis=1)
    jaggedness = loguniform_draw(random_subkeys[4], (number_of_heads, SEQUENCE_LENGTH), 0.5, 1.5)
    spike_positions = jax.random.randint(random_subkeys[5], (number_of_heads, 3), 0, SEQUENCE_LENGTH)
    spike_length = jax.random.uniform(random_subkeys[6], (number_of_heads, 3), jnp.float32, 0.22, 0.45)
    token_positions = jnp.arange(SEQUENCE_LENGTH, dtype=jnp.int32)
    match_count = token_positions[None, :, None] == spike_positions[:, None, :]
    spike_events = jnp.sum(jnp.where(match_count, spike_length[:, None, :], 0.0), axis=2)
    return -(learning_rate * block_multiplier * jaggedness) - spike_events


def draw_score_scale(key, part):
    return loguniform_draw(jax.random.fold_in(key, 11), (AHEADS,), 0.5, 8.0)


def draw_input_shift(key, part):
    return jax.random.uniform(jax.random.fold_in(key, 12), (MHEADS,), jnp.float32, -3.0, 1.0)


def draw_attention_decay(key, part):
    return jnp.cumsum(decay_steps(jax.random.fold_in(key, 13), AHEADS), axis=1)


def draw_memory_decay(key, part):
    return decay_steps(jax.random.fold_in(key, 14), MHEADS)


def shard_levels(rng, shape, cuts, least, largest):
    def one(dim, shards_of):
        heights = jax.random.uniform(jax.random.fold_in(jax.random.fold_in(rng, 6), dim), (shards_of,), jnp.float32, least / len(cuts), largest / len(cuts))
        return jnp.repeat(jnp.exp(heights), shape[dim] // shards_of).reshape((-1,) + (1,) * (len(shape) - dim - 1))

    factor_of = one(*cuts[0])
    for cut in cuts[1:]:
        factor_of = factor_of * one(*cut)
    return factor_of


def scatter_about(rng, shape, deviation, bound, pieces=(), kind=jnp.bfloat16):
    result = jax.random.normal(rng, shape, jnp.float32) * deviation
    if len(pieces) > 0:
        result = shard_levels(rng, shape, pieces, -0.22, 0.18) * result
    return jnp.clip(result, min=-bound, max=bound).astype(kind)


def setup_inputs(seed: int = 0) -> dict:
    seeds = jax.random.split(jax.random.key(seed), 21)
    tokens = draw_tokens(jax.random.fold_in(seeds[20], 71), 0)
    norm_gain = draw_norm_gain(jax.random.fold_in(seeds[20], 71), 0)
    attn_query = draw_attn_query(jax.random.fold_in(seeds[20], 71), 0)
    attn_key = draw_attn_key(jax.random.fold_in(seeds[20], 71), 0)
    attn_value = scatter_about(seeds[4], (D, AHEADS * ADIM), D ** -0.5, 0.125, ((1, 8),))
    score_scale = draw_score_scale(jax.random.fold_in(seeds[20], 71), 0)
    attention_decay = draw_attention_decay(jax.random.fold_in(seeds[20], 71), 0)
    mem_query = scatter_about(seeds[7], (D, MHEADS * MDIM), D ** -0.5, 0.125, ((1, 8),))
    mem_key = scatter_about(seeds[8], (D, MHEADS * MDIM), D ** -0.5, 0.125, ((1, 8),))
    mem_value = scatter_about(seeds[9], (D, MHEADS * MDIM), D ** -0.5, 0.125, ((1, 8),))
    mem_ingate = scatter_about(seeds[10], (D, MHEADS), D ** -0.5, 0.125)
    input_shift = draw_input_shift(jax.random.fold_in(seeds[20], 71), 0)
    memory_decay = draw_memory_decay(jax.random.fold_in(seeds[20], 71), 0)
    mem_outgate = scatter_about(seeds[13], (D, MHEADS * MDIM), D ** -0.5, 0.125, ((1, 8),))
    init_memory = scatter_about(seeds[14], (MHEADS, MDIM, MDIM), 32.0, 192.0, ((0, 8),), jnp.float32)
    init_normalizer = scatter_about(seeds[15], (MHEADS, MDIM), 32.0, 192.0, ((0, 8),), jnp.float32)
    attn_gain = jnp.clip(1.0 + 0.18 * jax.random.normal(seeds[16], (AHEADS * ADIM,), jnp.float32), 0.1, 1.9)
    mem_gain = jnp.clip(1.0 + 0.18 * jax.random.normal(seeds[17], (MHEADS * MDIM,), jnp.float32), 0.1, 1.9)
    attn_out = scatter_about(seeds[18], (AHEADS * ADIM, D), (AHEADS * ADIM + MHEADS * MDIM) ** -0.5, 0.125)
    mem_out = scatter_about(seeds[19], (MHEADS * MDIM, D), (AHEADS * ADIM + MHEADS * MDIM) ** -0.5, 0.125)
    return {"tokens": tokens, "norm_gain": norm_gain, "attn_query": attn_query, "attn_key": attn_key, "attn_value": attn_value, "score_scale": score_scale, "attention_decay": attention_decay, "mem_query": mem_query, "mem_key": mem_key, "mem_value": mem_value, "mem_ingate": mem_ingate, "input_shift": input_shift, "memory_decay": memory_decay, "mem_outgate": mem_outgate, "init_memory": init_memory, "init_normalizer": init_normalizer, "attn_gain": attn_gain, "mem_gain": mem_gain, "attn_out": attn_out, "mem_out": mem_out}


epsilon = 1e-06
highest = lax.Precision.HIGHEST

def rms_scale(values):
    return values * lax.rsqrt(lax.optimization_barrier(jnp.mean(values * values, axis=-1, keepdims=True)) + epsilon)

def attend_head(operands):
    query_rows, key_rows, value_rows, head_scale, cumulative = operands
    token_positions = jnp.arange(SEQUENCE_LENGTH, dtype=jnp.int32)

    def one_block(block_index):
        offset = block_index * TOK_DEV
        query_block = lax.dynamic_slice_in_dim(query_rows, offset, TOK_DEV, 0)
        decay_block = lax.dynamic_slice_in_dim(cumulative, offset, TOK_DEV, 0)
        scores = jnp.dot(query_block, key_rows.T, preferred_element_type=jnp.float32)
        scores = scores * (head_scale * ADIM ** (-0.5)) + decay_block[:, None] - cumulative[None, :]
        query_pos = offset + jnp.arange(TOK_DEV, dtype=jnp.int32)
        visible = token_positions[None, :] <= query_pos[:, None]
        row_top = lax.optimization_barrier(jnp.max(jnp.where(visible, scores, -jnp.inf), axis=1, keepdims=True))
        weights = jnp.where(visible, jnp.exp(jnp.where(visible, scores - row_top, 0.0)), 0.0)
        totals = lax.optimization_barrier(jnp.sum(weights, axis=1, keepdims=True))
        return jnp.dot(weights.astype(jnp.bfloat16), value_rows, preferred_element_type=jnp.float32) / totals
    return lax.map(one_block, jnp.arange(N_SP, dtype=jnp.int32)).reshape(SEQUENCE_LENGTH, ADIM)

def block_output(q_blocks, k_blocks, v_blocks, forget_cum, gate_blocks, mem_prev, norm_prev, stab_prev):
    block_len = q_blocks.shape[-2]
    causal = jnp.tril(jnp.ones((block_len, block_len), dtype=bool))
    log_pair = jnp.where(causal, forget_cum[..., :, None] - forget_cum[..., None, :] + gate_blocks[..., None, :], -jnp.inf)
    carried_log = forget_cum + stab_prev[..., None]
    row_top = jnp.maximum(carried_log, lax.optimization_barrier(jnp.max(log_pair, axis=-1)))
    pair_weight = jnp.einsum('hcld,hcsd->hcls', q_blocks, k_blocks, precision=highest) * jnp.exp(log_pair - row_top[..., None])
    carried_weight = jnp.exp(carried_log - row_top)
    numer = jnp.einsum('hcls,hcsd->hcld', pair_weight, v_blocks, precision=highest)
    numer = numer + carried_weight[..., None] * jnp.einsum('hcld,hcde->hcle', q_blocks, mem_prev, precision=highest)
    denom = lax.optimization_barrier(jnp.sum(pair_weight, axis=-1)) + carried_weight * jnp.einsum('hcld,hcd->hcl', q_blocks, norm_prev, precision=highest)
    return numer / jnp.maximum(jnp.abs(denom), jnp.exp(-row_top))[..., None]

def memory_cell(queries, keys_in, values_in, in_gate, log_forget, start_memory, start_norm):
    number_of_heads = queries.shape[0]
    block_count = SEQUENCE_LENGTH // BLOCK
    q_blocks = queries.reshape(number_of_heads, block_count, BLOCK, MDIM)
    k_blocks = keys_in.reshape(number_of_heads, block_count, BLOCK, MDIM)
    v_blocks = values_in.reshape(number_of_heads, block_count, BLOCK, MDIM)
    gate_blocks = in_gate.reshape(number_of_heads, block_count, BLOCK)
    forget_cum = jnp.cumsum(log_forget.reshape(number_of_heads, block_count, BLOCK), axis=-1)
    weight_log = forget_cum[..., -1:] - forget_cum + gate_blocks
    block_decay = forget_cum[..., -1]

    def advance(running, inputs):
        memory, normalizer, stabilizer = running
        key_block, value_block, log_block, decay_total = inputs
        new_stab = jnp.maximum(decay_total + stabilizer, lax.optimization_barrier(jnp.max(log_block, axis=-1)))
        shrink = jnp.exp(decay_total + stabilizer - new_stab)
        scaled = jnp.exp(log_block - new_stab[:, None])
        memory_new = shrink[:, None, None] * memory + jnp.einsum('hl,hld,hle->hde', scaled, key_block, value_block, precision=highest)
        norm_new = shrink[:, None] * normalizer + jnp.einsum('hl,hld->hd', scaled, key_block, precision=highest)
        return ((memory_new, norm_new, new_stab), (memory, normalizer, stabilizer))
    start_state = (start_memory, start_norm, jnp.zeros((number_of_heads,), jnp.float32))
    sequence_inputs = (jnp.moveaxis(k_blocks, 1, 0), jnp.moveaxis(v_blocks, 1, 0), jnp.moveaxis(weight_log, 1, 0), jnp.moveaxis(block_decay, 1, 0))
    _, (mem_prev, norm_prev, stab_prev) = lax.scan(advance, start_state, sequence_inputs)
    mem_prev = jnp.moveaxis(mem_prev, 0, 1)
    norm_prev = jnp.moveaxis(norm_prev, 0, 1)
    stab_prev = jnp.moveaxis(stab_prev, 0, 1)
    recalled = block_output(q_blocks, k_blocks, v_blocks, forget_cum, gate_blocks, mem_prev, norm_prev, stab_prev)
    return recalled.reshape(number_of_heads, SEQUENCE_LENGTH, MDIM)

def reference(tokens, norm_gain, attn_query, attn_key, attn_value, score_scale, attention_decay, mem_query, mem_key, mem_value, mem_ingate, input_shift, memory_decay, mem_outgate, init_memory, init_normalizer, attn_gain, mem_gain, attn_out, mem_out):
    normed = (rms_scale(tokens.astype(jnp.float32)) * norm_gain).astype(jnp.bfloat16)

    def project(weight_matrix):
        return jnp.dot(normed, weight_matrix, preferred_element_type=jnp.float32).astype(jnp.bfloat16)
    query_hat = rms_scale(project(attn_query).astype(jnp.float32).reshape(SEQUENCE_LENGTH, AHEADS, ADIM)).astype(jnp.bfloat16)
    key_hat = rms_scale(project(attn_key).astype(jnp.float32).reshape(SEQUENCE_LENGTH, AHEADS, ADIM)).astype(jnp.bfloat16)
    att_values = project(attn_value).reshape(SEQUENCE_LENGTH, AHEADS, ADIM)
    attended = lax.map(attend_head, (query_hat.transpose(1, 0, 2), key_hat.transpose(1, 0, 2), att_values.transpose(1, 0, 2), score_scale, attention_decay))
    attended_rows = attended.transpose(1, 0, 2).reshape(SEQUENCE_LENGTH, AHEADS * ADIM)
    att_mix = (rms_scale(attended_rows) * attn_gain).astype(jnp.bfloat16)

    def heads_first(matrix):
        return matrix.astype(jnp.float32).reshape(SEQUENCE_LENGTH, MHEADS, MDIM).transpose(1, 0, 2)
    mem_queries = heads_first(project(mem_query)) * MDIM ** (-0.5)
    mem_keys = heads_first(project(mem_key))
    mem_values = heads_first(project(mem_value))
    in_gate = (jnp.dot(normed, mem_ingate, preferred_element_type=jnp.float32) + input_shift).T
    recalled = memory_cell(mem_queries, mem_keys, mem_values, in_gate, memory_decay, init_memory, init_normalizer)
    recalled_rows = recalled.transpose(1, 0, 2).reshape(SEQUENCE_LENGTH, MHEADS * MDIM)
    out_gate = jax.nn.sigmoid(project(mem_outgate).astype(jnp.float32))
    mem_mix = (rms_scale(recalled_rows) * mem_gain * out_gate).astype(jnp.bfloat16)
    mixed = jnp.dot(att_mix, attn_out, preferred_element_type=jnp.float32) + jnp.dot(mem_mix, mem_out, preferred_element_type=jnp.float32)
    return mixed.astype(jnp.bfloat16)
```

```python
import functools
import math

import jax
import jax.numpy as jnp
from jax import lax
from jax.experimental import pallas as pl
from jax.experimental.pallas import tpu as pltpu
from jax.sharding import PartitionSpec as P

MESH = pl.DeviceIdType.MESH
f32 = jnp.float32
bf16 = jnp.bfloat16
EPS = 1e-06
LOG2E = math.log2(math.e)
FAR = -1e30
ROWS = 1024
AD = 64
MD = 128
QT = 256
N_SP, N_TP = 16, 8
VEXT = AD + 16
ZR = MD + 16


def dot(a, b):
    return jnp.dot(a, b, preferred_element_type=f32)


def pieces(x):
    hi = x.astype(bf16).astype(f32)
    rest = x - hi
    mid = rest.astype(bf16).astype(f32)
    low = (rest - mid).astype(bf16).astype(f32)
    return hi, mid, low


def halves(x):
    hi = x.astype(bf16)
    return hi, (x - hi.astype(f32)).astype(bf16)


def rows_of(values, height, width):
    at = lax.broadcasted_iota(jnp.int32, (height, width), 0)
    out = jnp.zeros((height, width), f32)
    for n, value in enumerate(values):
        out = jnp.where(at == n, value, out)
    return out


def project_kernel(tok, gain, wq, wk, wv, wmq, wmk, wmv, wmo, ing, shift,
                   q_o, kv_o, mq_o, mk_o, mv_o, mo_o, gate_o, w, sems):
    @pl.when(pl.program_id(0) == 0)
    def _():
        copies = []
        for n, (ref, at) in enumerate(
            ((wq, 0), (wk, 1), (wv, 2), (wmk, 3), (wmq, 4), (wmv, 5), (wmo, 6))
        ):
            copy = pltpu.make_async_copy(ref, w.at[:, at * 128 : at * 128 + 128], sems.at[n])
            copy.start()
            copies.append(copy)
        w[:, 896:1024] = jnp.zeros((2048, 128), bf16)
        w[:, 896:904] = ing[...]
        for copy in copies:
            copy.wait()

    x = tok[...].astype(f32)
    ms = jnp.mean(x * x, axis=-1, keepdims=True)
    n = (x * lax.rsqrt(ms + EPS) * gain[...]).astype(bf16)

    def unit(v):
        return (v * lax.rsqrt(jnp.mean(v * v, axis=0, keepdims=True) + EPS)).astype(bf16)

    def turned(p):
        return p.astype(bf16).astype(f32).T

    p = dot(n, w[:, 0:256])
    q, k = turned(p[:, :128]), turned(p[:, 128:])
    for h in range(2):
        q_o[h] = unit(q[h * AD : h * AD + AD])
        kv_o[h, 0:AD] = unit(k[h * AD : h * AD + AD])
    p = dot(n, w[:, 256:512])
    v = turned(p[:, :128]).astype(bf16)
    for h in range(2):
        kv_o[h, AD : 2 * AD] = v[h * AD : h * AD + AD]
    mk_o[...] = p[:, 128:].astype(bf16)
    p = dot(n, w[:, 512:768])
    mq_o[...] = turned(p[:, :128]).astype(bf16)
    mv_o[...] = turned(p[:, 128:]).astype(bf16)
    p = dot(n, w[:, 768:1024])
    mo_o[...] = turned(p[:, :128]).astype(bf16)
    gate_o[...] = p[:, 128:].T[0:8] + shift[...]


def project(tokens, gain, weights, ingate, shift):
    tile = 256
    hbm = pl.BlockSpec(memory_space=pl.ANY)

    def whole(shape):
        return pl.BlockSpec(shape, lambda i: (0,) * len(shape))

    lanes = lambda *lead: pl.BlockSpec((*lead, tile), lambda i: (0,) * len(lead) + (i,))
    return pl.pallas_call(
        project_kernel,
        grid=(ROWS // tile,),
        in_specs=[pl.BlockSpec((tile, 2048), lambda i: (i, 0)), whole((1, 2048))]
        + [hbm] * 7
        + [whole((2048, 8)), whole((8, 1))],
        out_specs=[
            lanes(2, AD), lanes(2, 2 * AD), lanes(MD),
            pl.BlockSpec((tile, MD), lambda i: (i, 0)),
            lanes(MD), lanes(MD), lanes(8),
        ],
        out_shape=[
            jax.ShapeDtypeStruct((2, AD, ROWS), bf16),
            jax.ShapeDtypeStruct((2, 2 * AD, ROWS), bf16),
            jax.ShapeDtypeStruct((MD, ROWS), bf16),
            jax.ShapeDtypeStruct((ROWS, MD), bf16),
            jax.ShapeDtypeStruct((MD, ROWS), bf16),
            jax.ShapeDtypeStruct((MD, ROWS), bf16),
            jax.ShapeDtypeStruct((8, ROWS), f32),
        ],
        scratch_shapes=[pltpu.VMEM((2048, 1024), bf16), pltpu.SemaphoreType.DMA((7,))],
        compiler_params=pltpu.CompilerParams(vmem_limit_bytes=48 * 2**20),
        cost_estimate=pl.CostEstimate(
            flops=2 * ROWS * 2048 * 1024, bytes_accessed=12 * 2**20, transcendentals=0
        ),
    )(tokens, gain, *weights, ingate, shift)


def shifted(x, by, fill):
    at = lax.broadcasted_iota(jnp.int32, x.shape, 1)
    return jnp.where(at >= by, pltpu.roll(x, by, 1), fill)


def scan_lanes(x, join, fill):
    by = 1
    while by < x.shape[1]:
        x = join(x, shifted(x, by, fill))
        by *= 2
    return x


def mix_kernel(scale_ref, q_in, kv_in, mq_in, mk_in, mv_in, mo_in, gate_in, fade_in, decay_in,
               cinit_in, ninit_in, again_in, mgain_in, wa_in, wm_in, out,
               wa, wm, kv, qb, decays, kaug, qaug, best, acc, ostage, att,
               zstage, zb, mstage, mb, mext, mnum,
               wsem, dsem, kv_s, kv_r, q_s, q_r, z_s, z_r, m_s, m_r, o_s, o_r, f_s, d_s, d_r):
    r = lax.axis_index("sp")
    t = lax.axis_index("tp")
    x, k = t // 2, t % 2
    g, a = r // 4, r % 4
    b = k
    hi = jnp.where(b == 0, 15 - a, 8 + a)
    lo = jnp.where(b == 0, a, 7 - a)
    both_to = 8 + a
    head = 4 * x + g

    barrier = pltpu.get_barrier_semaphore()
    me = r * N_TP + t

    def greet(n, _):
        other = (me + n) % (N_SP * N_TP)
        pl.semaphore_signal(
            barrier, inc=1, device_id=(other // N_TP, other % N_TP), device_id_type=MESH
        )
        return 0

    lax.fori_loop(1, N_SP * N_TP, greet, 0)

    w_copies = [
        pltpu.make_async_copy(wa_in, wa, wsem.at[0]),
        pltpu.make_async_copy(wm_in, wm, wsem.at[1]),
    ]
    for copy in w_copies:
        copy.start()
    own_decay = pltpu.make_async_copy(decay_in, decays.at[k], dsem)
    own_decay.start()

    gate = jnp.sum(
        jnp.where(lax.broadcasted_iota(jnp.int32, (8, ROWS), 0) == t, gate_in[...], 0.0),
        axis=0, keepdims=True,
    )
    fade = scan_lanes(jnp.broadcast_to(fade_in[...], (8, ROWS)), jnp.add, 0.0)
    level = jnp.broadcast_to(gate, (8, ROWS)) - fade
    crest8 = scan_lanes(level, jnp.maximum, FAR)
    crest = crest8[0:1]
    top = crest[:, ROWS - 1 : ROWS]
    total = fade[0:1, ROWS - 1 : ROWS]
    mext[0:MD] = mv_in[...]
    mext[MD:ZR] = jnp.ones((16, ROWS), bf16)
    weighted = mext[...].astype(f32) * jnp.exp(level[0:1] - top)
    w_hi, w_lo = halves(weighted)
    z = dot(w_hi, mk_in[...]) + dot(w_lo, mk_in[...])
    zstage[0:MD] = z[0:MD].astype(bf16)
    z_rest = (
        *pieces(z[MD : MD + 1]),
        *pieces(jnp.broadcast_to(total + top, (1, MD))),
        *pieces(jnp.broadcast_to(total, (1, MD))),
    )
    zstage[MD:ZR] = rows_of(z_rest, 16, MD).astype(bf16)

    pl.semaphore_wait(barrier, N_SP * N_TP - 1)

    def decay_copy():
        return pltpu.make_async_remote_copy(
            decay_in, decays.at[k], d_s, d_r, device_id=(r, 2 * x + 1 - k), device_id_type=MESH
        )

    decay_copy().start()

    def worker(chunk):
        quarter, low = chunk // 4, chunk % 4
        wa_ = jnp.where(quarter % 2 == 0, low, 3 - low)
        wb = jnp.where((quarter == 0) | (quarter == 3), 0, 1)
        slot = jnp.where(quarter >= 2, 0, 1)
        return wa_, wb, slot

    my_a, my_b, my_slot = worker(r)

    def q_copy(h):
        sp, tp = 4 * (2 * k + h) + my_a, 2 * x + my_b
        own = (sp == r) & (tp == t)
        return own, pltpu.make_async_remote_copy(
            q_in.at[h], qb.at[my_slot], q_s.at[h], q_r.at[my_slot],
            device_id=(sp, tp), device_id_type=MESH,
        )

    def kv_copy(h, to_a):
        sp = 4 * (2 * k + h) + to_a
        core = jnp.where(r <= 8 + to_a, r % 2, 0)
        tp = 2 * x + core
        own = (sp == r) & (tp == t)
        return (r <= 15 - to_a), own, pltpu.make_async_remote_copy(
            kv_in.at[h], kv.at[r, 0 : 2 * AD], kv_s.at[h * 4 + to_a], kv_r.at[r],
            device_id=(sp, tp), device_id_type=MESH,
        )

    for h in range(2):
        own, copy = q_copy(h)

        @pl.when(jnp.logical_not(own))
        def _():
            copy.start()

        @pl.when(own)
        def _():
            qb[my_slot] = q_in[h]

    def z_copy(to):
        return pltpu.make_async_remote_copy(
            zstage, zb.at[r], z_s.at[to], z_r.at[r], device_id=(to, t), device_id_type=MESH
        )

    def z_send(to, _):
        z_copy(to).start()
        return 0

    lax.fori_loop(r + 1, N_SP, z_send, 0)

    for h in range(2):
        for to_a in range(4):
            used, own, copy = kv_copy(h, to_a)

            @pl.when(used & jnp.logical_not(own))
            def _():
                copy.start()

            @pl.when(used & own)
            def _():
                kv[r, 0 : 2 * AD] = kv_in[h]

    levels = level.T
    for j in range(ROWS // QT):
        cols = slice(j * QT, j * QT + QT)
        n_keys = j * QT + QT
        raw = dot(mk_in[0:n_keys], mq_in[:, cols]) * MD**-0.5
        log = levels[0:n_keys, 0:1] - crest[:, cols]
        key_at = lax.broadcasted_iota(jnp.int32, (n_keys, QT), 0)
        query_at = lax.broadcasted_iota(jnp.int32, (n_keys, QT), 1) + j * QT
        seen = key_at <= query_at
        pair = jnp.where(seen, raw * jnp.exp(jnp.where(seen, log, 0.0)), 0.0)
        p_hi, p_lo = halves(pair)
        mnum[:, cols] = dot(mext[:, 0:n_keys], p_hi) + dot(mext[:, 0:n_keys], p_lo)

    own_decay.wait()
    decay_copy().wait_recv()
    factor = scale_ref[head] * (AD**-0.5 * LOG2E)

    def decay_of(chunk):
        slab = decays[g // 2, :, pl.ds(pl.multiple_of(chunk * ROWS, ROWS), ROWS)]
        return jnp.where(g % 2 == 0, slab[0:1], slab[1:2]) * LOG2E

    for slot in range(2):
        chunk = hi if slot == 0 else lo
        own = (chunk == r) & (g // 2 == k)

        @pl.when(jnp.logical_not(own))
        def _():
            pltpu.make_async_remote_copy(
                q_in.at[0], qb.at[slot], q_s.at[0], q_r.at[slot],
                device_id=(r, 2 * x + 1 - k), device_id_type=MESH,
            ).wait_recv()

        q_hi, q_mid, q_lo = pieces(qb[slot].astype(f32) * factor)
        d_hi, d_mid, d_lo = pieces(decay_of(chunk))
        qaug[slot, 0:64] = q_hi.astype(bf16)
        qaug[slot, 64:80] = rows_of((-1.0, -1.0, -1.0, d_hi, d_mid, d_lo), 16, ROWS).astype(bf16)
        qaug[slot, 80:128] = jnp.zeros((48, ROWS), bf16)
        qaug[slot, 128:192] = q_mid.astype(bf16)
        qaug[slot, 192:256] = q_lo.astype(bf16)
        best[slot] = jnp.full((8, ROWS), FAR, f32)
        acc[slot] = jnp.zeros((VEXT, ROWS), f32)

    def ones_row(chunk, _):
        kv[chunk, 2 * AD : 2 * AD + 16] = jnp.ones((16, ROWS), bf16)
        return 0

    lax.fori_loop(0, hi + 1, ones_row, 0)

    def forward_copy(chunk):
        return pltpu.make_async_remote_copy(
            kv.at[chunk, 0 : 2 * AD], kv.at[chunk, 0 : 2 * AD], f_s.at[chunk], kv_r.at[chunk],
            device_id=(r, 2 * x + 1 - k), device_id_type=MESH,
        )

    def forwards(chunk):
        return (chunk <= both_to) & (chunk % 2 == b)

    def arrive(chunk):
        own = (chunk == r) & (g // 2 == k) & (jnp.where(chunk <= both_to, chunk % 2, 0) == b)

        @pl.when(jnp.logical_not(own))
        def _():
            forward_copy(chunk).wait_recv()

        @pl.when(forwards(chunk))
        def _():
            forward_copy(chunk).start()

    def fold(slot, chunk, diag):
        def scores(i):
            n_keys = (i + 1) * QT if diag else ROWS
            s = dot(kaug[0:n_keys], qaug[slot, :, i * QT : i * QT + QT])
            if diag:
                key_at = lax.broadcasted_iota(jnp.int32, (n_keys, QT), 0)
                query_at = lax.broadcasted_iota(jnp.int32, (n_keys, QT), 1) + i * QT
                s = jnp.where(key_at <= query_at, s, FAR)
            return s

        def finish(i, s):
            cols = slice(i * QT, i * QT + QT)
            n_keys = s.shape[0]
            old = best[slot, 0:1, cols]
            new = jnp.maximum(old, jnp.max(s, axis=0, keepdims=True))
            weights = jnp.exp2(s - new).astype(bf16)
            got = dot(kv[chunk, AD : AD + VEXT, 0:n_keys], weights)
            acc[slot, :, cols] = acc[slot, :, cols] * jnp.exp2(old - new) + got
            best[slot, 0:1, cols] = new

        tiles = ROWS // QT
        s = scores(0)
        for i in range(tiles):
            later = scores(i + 1) if i + 1 < tiles else None
            finish(i, s)
            s = later

    arrive(0)

    def visit(chunk, _):
        @pl.when(chunk < hi)
        def _():
            arrive(chunk + 1)

        keys = kv[chunk, 0:AD]
        keys32 = keys.astype(f32)
        d_hi, d_mid, d_lo = pieces(decay_of(chunk))
        extra = rows_of((d_hi, d_mid, d_lo, 1.0, 1.0, 1.0), 64, ROWS)
        kaug[:, 0:128] = jnp.concatenate([keys32, extra], axis=0).T.astype(bf16)
        kaug[:, 128:256] = jnp.concatenate([keys32, keys32], axis=0).T.astype(bf16)

        def side(slot, _):
            mine = jnp.where(slot == 0, hi, lo)

            @pl.when(chunk < mine)
            def _():
                fold(slot, chunk, False)

            @pl.when(chunk == mine)
            def _():
                fold(slot, chunk, True)

            return 0

        lax.fori_loop(0, 2, side, 0)
        return 0

    lax.fori_loop(0, hi + 1, visit, 0)

    def o_copy(slot, p):
        chunk = hi if slot == 0 else lo
        own = (chunk == r) & (p == t)
        return own, pltpu.make_async_remote_copy(
            ostage.at[slot, p], att.at[head], o_s.at[slot, p], o_r.at[head],
            device_id=(chunk, p), device_id_type=MESH,
        )

    for slot in range(2):
        result = acc[slot, 0:AD] / acc[slot, AD : AD + 1]
        result = result.astype(bf16)
        for p in range(N_TP):
            ostage[slot, p] = result[:, p * 128 : p * 128 + 128]

        def o_send(p, _):
            own, copy = o_copy(slot, p)

            @pl.when(jnp.logical_not(own))
            def _():
                copy.start()

            @pl.when(own)
            def _():
                att[head] = ostage[slot, p]

            return 0

        lax.fori_loop(0, N_TP, o_send, 0)

    z0 = jnp.concatenate(
        [cinit_in[0].T, jnp.broadcast_to(ninit_in[...], (16, MD))], axis=0
    )

    def enter(n, carry):
        state, log = carry
        pltpu.make_async_remote_copy(
            zstage, zb.at[n], z_s.at[0], z_r.at[n], device_id=(0, t), device_id_type=MESH
        ).wait_recv()
        rest = zb[n, MD:ZR].astype(f32)
        norm = rest[0:1] + rest[1:2] + rest[2:3]
        stab = rest[3:4] + rest[4:5] + rest[5:6]
        faded = log + (rest[6:7] + rest[7:8] + rest[8:9])
        new = jnp.maximum(faded, stab)
        added = jnp.concatenate(
            [zb[n, 0:MD].astype(f32), jnp.broadcast_to(norm, (16, MD))], axis=0
        )
        return state * jnp.exp(faded - new) + added * jnp.exp(stab - new), new

    state, log = lax.fori_loop(0, r, enter, (z0, jnp.zeros((1, MD), f32)))
    log = log[:, 0:1]
    peak = jnp.maximum(crest, log)
    s_hi, s_lo = halves(state)
    carried = (dot(s_hi, mq_in[...]) + dot(s_lo, mq_in[...])) * MD**-0.5
    numer = mnum[...] * jnp.exp(crest - peak) + carried * jnp.exp(log - peak)
    floor = jnp.exp(-(fade[0:1] + peak))
    recalled = numer[0:MD] / jnp.maximum(jnp.abs(numer[MD : MD + 1]), floor)
    squares = jnp.sum(recalled * recalled, axis=0, keepdims=True)
    sq_hi, sq_mid, sq_lo = pieces(squares)
    gated = (recalled * jax.nn.sigmoid(mo_in[...].astype(f32))).astype(bf16)
    stats = rows_of((sq_hi, sq_mid, sq_lo), 16, ROWS).astype(bf16)
    for p in range(N_TP):
        mstage[p, 0:MD] = gated[:, p * 128 : p * 128 + 128]
        mstage[p, MD:ZR] = stats[:, p * 128 : p * 128 + 128]

    def m_copy(p):
        return pltpu.make_async_remote_copy(
            mstage.at[p], mb.at[t], m_s.at[p], m_r.at[t], device_id=(r, p), device_id_type=MESH
        )

    def m_send(p, _):
        @pl.when(p != t)
        def _():
            m_copy(p).start()

        @pl.when(p == t)
        def _():
            mb[t] = mstage[p]

        return 0

    lax.fori_loop(0, N_TP, m_send, 0)

    _, from_b, _ = worker(r)
    from_a, _, _ = worker(r)

    def o_wait(n, _):
        own = (n == head) & ((hi == r) | (lo == r))

        @pl.when(jnp.logical_not(own))
        def _():
            pltpu.make_async_remote_copy(
                ostage.at[0, 0], att.at[n], o_s.at[0, 0], o_r.at[n],
                device_id=(r, (t + 1) % N_TP), device_id_type=MESH,
            ).wait_recv()

        return 0

    def m_wait(n, _):
        @pl.when(n != t)
        def _():
            pltpu.make_async_remote_copy(
                mstage.at[0], mb.at[n], m_s.at[0], m_r.at[n],
                device_id=(r, (t + 1) % N_TP), device_id_type=MESH,
            ).wait_recv()

        return 0

    lax.fori_loop(0, N_TP, m_wait, 0)
    for copy in w_copies:
        copy.wait()

    m_all = jnp.concatenate([mb[n, 0:MD].astype(f32).T for n in range(N_TP)], axis=1)
    m_stats = sum(mb[n, MD:ZR].astype(f32) for n in range(N_TP)).T
    m_sq = m_stats[:, 0:1] + m_stats[:, 1:2] + m_stats[:, 2:3]
    m_mix = (m_all * lax.rsqrt(m_sq / 1024.0 + EPS) * mgain_in[...]).astype(bf16)

    lax.fori_loop(0, 16, o_wait, 0)
    a_all = jnp.concatenate(
        [
            jnp.concatenate([att[2 * n], att[2 * n + 1]], axis=0).astype(f32).T
            for n in range(8)
        ],
        axis=1,
    )
    a_sq = jnp.sum(a_all * a_all, axis=1, keepdims=True)
    a_mix = (a_all * lax.rsqrt(a_sq / 1024.0 + EPS) * again_in[...]).astype(bf16)
    for n in range(4):
        cols = slice(n * 512, n * 512 + 512)
        out[:, cols] = (dot(m_mix, wm[:, cols]) + dot(a_mix, wa[:, cols])).astype(bf16)

    decay_copy().wait_send()
    for h in range(2):
        own, copy = q_copy(h)

        @pl.when(jnp.logical_not(own))
        def _():
            copy.wait_send()

        for to_a in range(4):
            used, own, copy = kv_copy(h, to_a)

            @pl.when(used & jnp.logical_not(own))
            def _():
                copy.wait_send()

    def z_done(to, _):
        z_copy(to).wait_send()
        return 0

    lax.fori_loop(r + 1, N_SP, z_done, 0)

    def f_done(chunk, _):
        @pl.when(forwards(chunk))
        def _():
            forward_copy(chunk).wait_send()

        return 0

    lax.fori_loop(0, hi + 1, f_done, 0)

    def p_done(p, _):
        for slot in range(2):
            own, copy = o_copy(slot, p)

            @pl.when(jnp.logical_not(own))
            def _():
                copy.wait_send()

        @pl.when(p != t)
        def _():
            m_copy(p).wait_send()

        return 0

    lax.fori_loop(0, N_TP, p_done, 0)


def mix(*arrays):
    vmem = pl.BlockSpec(memory_space=pltpu.VMEM)
    hbm = pl.BlockSpec(memory_space=pl.ANY)
    dma = pltpu.SemaphoreType.DMA
    return pl.pallas_call(
        mix_kernel,
        out_shape=jax.ShapeDtypeStruct((128, 2048), bf16),
        in_specs=[pl.BlockSpec(memory_space=pltpu.SMEM)] + [vmem] * 8 + [hbm]
        + [vmem] * 4 + [hbm] * 2,
        out_specs=vmem,
        scratch_shapes=[
            pltpu.VMEM((1024, 2048), bf16),
            pltpu.VMEM((1024, 2048), bf16),
            pltpu.VMEM((N_SP, 2 * AD + 16, ROWS), bf16),
            pltpu.VMEM((2, AD, ROWS), bf16),
            pltpu.VMEM((2, 2, N_SP * ROWS), f32),
            pltpu.VMEM((ROWS, 256), bf16),
            pltpu.VMEM((2, 256, ROWS), bf16),
            pltpu.VMEM((2, 8, ROWS), f32),
            pltpu.VMEM((2, VEXT, ROWS), f32),
            pltpu.VMEM((2, N_TP, AD, 128), bf16),
            pltpu.VMEM((16, AD, 128), bf16),
            pltpu.VMEM((ZR, MD), bf16),
            pltpu.VMEM((N_SP, ZR, MD), bf16),
            pltpu.VMEM((N_TP, ZR, 128), bf16),
            pltpu.VMEM((N_TP, ZR, 128), bf16),
            pltpu.VMEM((ZR, ROWS), bf16),
            pltpu.VMEM((ZR, ROWS), f32),
            dma((2,)), dma,
            dma((8,)), dma((N_SP,)),
            dma((2,)), dma((2,)),
            dma((N_SP,)), dma((N_SP,)),
            dma((N_TP,)), dma((N_TP,)),
            dma((2, N_TP)), dma((16,)),
            dma((N_SP,)), dma, dma,
        ],
        compiler_params=pltpu.CompilerParams(
            collective_id=0, has_side_effects=True, vmem_limit_bytes=60 * 2**20
        ),
        cost_estimate=pl.CostEstimate(
            flops=60 * 10**9, bytes_accessed=12 * 2**20, transcendentals=0
        ),
    )(*arrays)


def on_device(tokens, norm_gain, attn_query, attn_key, attn_value, score_scale, attention_decay,
              mem_query, mem_key, mem_value, mem_ingate, input_shift, memory_decay, mem_outgate,
              init_memory, init_normalizer, attn_gain, mem_gain, attn_out, mem_out):
    q, kv, mq, mk, mv, mo, gate = project(
        tokens, norm_gain.reshape(1, 2048),
        (attn_query, attn_key, attn_value, mem_query, mem_key, mem_value, mem_outgate),
        mem_ingate, input_shift.reshape(8, 1),
    )
    return mix(
        score_scale, q, kv, mq, mk, mv, mo, gate, memory_decay, attention_decay,
        init_memory, init_normalizer, attn_gain.reshape(1, 1024), mem_gain.reshape(1, 1024),
        attn_out, mem_out,
    )


def solution(mesh):
    tp = P(None, "tp")
    placed = (
        P("sp", None), P(), tp, tp, tp, P(), P("tp", None), tp, tp, tp, P(), P(),
        P("tp", "sp"), tp, P("tp", None, None), P("tp", None), P(), P(), P(), P(),
    )
    return jax.shard_map(
        on_device, mesh=mesh, in_specs=placed, out_specs=P(("sp", "tp"), None), check_vma=False
    )
```

```python
import functools
import math

import jax
import jax.numpy as jnp
from jax import lax
from jax.experimental import pallas as pl
from jax.experimental.pallas import tpu as pltpu
from jax.sharding import PartitionSpec as P

MESH = pl.DeviceIdType.MESH
f32 = jnp.float32
bf16 = jnp.bfloat16
EPS = 1e-06
LOG2E = math.log2(math.e)
FAR = -1e30
ROWS = 1024
AD = 64
MD = 128
QT = 256
N_SP, N_TP = 16, 8
VEXT = AD + 16
ZR = MD + 16


def dot(a, b):
    return jnp.dot(a, b, preferred_element_type=f32)


def pieces(x):
    hi = x.astype(bf16).astype(f32)
    rest = x - hi
    mid = rest.astype(bf16).astype(f32)
    low = (rest - mid).astype(bf16).astype(f32)
    return hi, mid, low


def halves(x):
    hi = x.astype(bf16)
    return hi, (x - hi.astype(f32)).astype(bf16)


def rows_of(values, height, width):
    at = lax.broadcasted_iota(jnp.int32, (height, width), 0)
    out = jnp.zeros((height, width), f32)
    for n, value in enumerate(values):
        out = jnp.where(at == n, value, out)
    return out


def shifted(x, by, fill):
    at = lax.broadcasted_iota(jnp.int32, x.shape, 1)
    return jnp.where(at >= by, pltpu.roll(x, by, 1), fill)


def scan_lanes(x, join, fill):
    by = 1
    while by < x.shape[1]:
        x = join(x, shifted(x, by, fill))
        by *= 2
    return x


def mix_kernel(scale_ref, shift_ref, tok_in, wq_in, wk_in, wv_in, wmq_in, wmk_in, wmv_in, wmo_in, ing_in,
               ngain_in, fade_hbm, decay_in, cinit_hbm, ninit_hbm, again_hbm, mgain_hbm, wa_in, wm_in,
               out, tok, w, ing, ngain, fade_in, cinit_in, ninit_in, again_in, mgain_in,
               qs, kvs, mq_in, mk_in, mo_in, fade_s, crest_s, levels,
               wa, wm, kv, qb, decays, kaug, qaug, best, acc, ostage, att,
               zstage, zb, mstage, mb, mext, mnum,
               isem, wsem, kv_s, kv_r, q_s, q_r, z_s, z_r, m_s, m_r, o_s, o_r, p_s, f_s, d_s, d_r):
    r = lax.axis_index("sp")
    t = lax.axis_index("tp")
    x, k = t // 2, t % 2
    rz, ry = r // 4, r % 4
    g = 2 * (rz // 2) + ry // 2
    a = 2 * (rz % 2) + ry % 2
    b = k
    hi = jnp.where(b == 0, 15 - a, 8 + a)
    lo = jnp.where(b == 0, a, 7 - a)
    head = 4 * x + g

    def chip_of(block, member):
        z = 2 * (block // 2) + member // 2
        y = 2 * (block % 2) + member % 2
        return 4 * z + y

    def flip(v):
        return v + 1 - 2 * (v % 2)

    def core_for(chunk):
        return (chunk % 4) // 2

    loads = []

    def load(src, dst):
        copy = pltpu.make_async_copy(src, dst, isem.at[len(loads)])
        copy.start()
        loads.append(copy)
        return copy

    small = [
        load(ngain_in, ngain), load(ing_in, ing), load(fade_hbm, fade_in), load(cinit_hbm, cinit_in),
        load(ninit_hbm, ninit_in), load(again_hbm, again_in), load(mgain_hbm, mgain_in),
    ]
    tok_loads = []
    first = []
    rest = []
    for i in range(4):
        rows = slice(i * 256, i * 256 + 256)
        tok_loads.append(load(tok_in.at[rows], tok.at[rows]))
        if i == 0:
            for n, ref in ((0, wq_in), (1, wk_in), (2, wv_in), (3, wmk_in)):
                first.append(load(ref, w.at[:, n * 128 : n * 128 + 128]))
    for n, ref in ((4, wmq_in), (5, wmv_in), (6, wmo_in)):
        rest.append(load(ref, w.at[:, n * 128 : n * 128 + 128]))
    own_decay = load(decay_in, decays.at[k])

    barrier = pltpu.get_barrier_semaphore()
    me = r * N_TP + t

    def greet(n, _):
        other = (me + n) % (N_SP * N_TP)
        pl.semaphore_signal(
            barrier, inc=1, device_id=(other // N_TP, other % N_TP), device_id_type=MESH
        )
        return 0

    lax.fori_loop(1, N_SP * N_TP, greet, 0)

    for copy in small:
        copy.wait()
    for copy in first:
        copy.wait()

    def unit(v):
        return (v * lax.rsqrt(jnp.mean(v * v, axis=0, keepdims=True) + EPS)).astype(bf16)

    def turned(p):
        return p.astype(bf16).astype(f32).T

    for i in range(4):
        rows = slice(i * 256, i * 256 + 256)
        tok_loads[i].wait()
        v = tok[rows].astype(f32)
        ms = jnp.mean(v * v, axis=-1, keepdims=True)
        n = (v * lax.rsqrt(ms + EPS) * ngain[...]).astype(bf16)
        tok[rows] = n
        p = dot(n, w[:, 0:256])
        pq, pk = turned(p[:, :128]), turned(p[:, 128:])
        for h in range(2):
            qs[h, :, rows] = unit(pq[h * AD : h * AD + AD])
            kvs[h, 0:AD, rows] = unit(pk[h * AD : h * AD + AD])
        p = dot(n, w[:, 256:512])
        pv = turned(p[:, :128]).astype(bf16)
        for h in range(2):
            kvs[h, AD : 2 * AD, rows] = pv[h * AD : h * AD + AD]
        mk_in[rows] = p[:, 128:].astype(bf16)

    pl.semaphore_wait(barrier, N_SP * N_TP - 1)

    def worker(chunk):
        quarter, low = chunk // 4, chunk % 4
        wa_ = jnp.where(quarter % 2 == 0, low, 3 - low)
        wb = jnp.where((quarter == 0) | (quarter == 3), 0, 1)
        slot = jnp.where(quarter >= 2, 0, 1)
        return wa_, wb, slot

    my_a, my_b, my_slot = worker(r)

    def q_copy(h):
        sp, tp = chip_of(2 * k + h, my_a), 2 * x + my_b
        own = (sp == r) & (tp == t)
        return own, pltpu.make_async_remote_copy(
            qs.at[h], qb.at[my_slot], q_s.at[h], q_r.at[my_slot],
            device_id=(sp, tp), device_id_type=MESH,
        )

    def kv_copy(h):
        block = 2 * k + h
        z = jnp.where(rz // 2 == block // 2, rz, 3 - rz)
        y = jnp.where(ry // 2 == block % 2, ry, 3 - ry)
        sp, tp = 4 * z + y, 2 * x + core_for(r)
        own = (sp == r) & (tp == t)
        return own, pltpu.make_async_remote_copy(
            kvs.at[h], kv.at[r, 0 : 2 * AD], kv_s.at[h], kv_r.at[r],
            device_id=(sp, tp), device_id_type=MESH,
        )

    for h in range(2):
        own, copy = kv_copy(h)

        @pl.when(jnp.logical_not(own))
        def _():
            copy.start()

        @pl.when(own)
        def _():
            kv[r, 0 : 2 * AD] = kvs[h]

    def decay_copy():
        return pltpu.make_async_remote_copy(
            decay_in, decays.at[k], d_s, d_r, device_id=(r, 2 * x + 1 - k), device_id_type=MESH
        )

    decay_copy().start()
    for h in range(2):
        own, copy = q_copy(h)

        @pl.when(jnp.logical_not(own))
        def _():
            copy.start()

        @pl.when(own)
        def _():
            qb[my_slot] = qs[h]

    w[:, 896:1024] = jnp.zeros((2048, 128), bf16)
    w[:, 896:904] = ing[...].astype(f32).T.astype(bf16)
    for copy in rest:
        copy.wait()
    gates = []
    for i in range(4):
        rows = slice(i * 256, i * 256 + 256)
        p = dot(tok[rows], w[:, 512:768])
        mq_in[:, rows] = turned(p[:, :128]).astype(bf16)
        mext[0:MD, rows] = turned(p[:, 128:]).astype(bf16)
        p = dot(tok[rows], w[:, 768:1024])
        mo_in[:, rows] = turned(p[:, :128]).astype(bf16)
        gates.append(p[:, 128:].T[0:8])

    gate8 = jnp.concatenate(gates, axis=1)
    gate = jnp.sum(
        jnp.where(lax.broadcasted_iota(jnp.int32, (8, ROWS), 0) == t, gate8, 0.0),
        axis=0, keepdims=True,
    ) + shift_ref[t]
    fade = scan_lanes(jnp.broadcast_to(fade_in[...], (8, ROWS)), jnp.add, 0.0)
    level = jnp.broadcast_to(gate, (8, ROWS)) - fade
    crest8 = scan_lanes(level, jnp.maximum, FAR)
    fade_s[...] = fade
    crest_s[...] = crest8
    levels[...] = level.T
    crest = crest8[0:1]
    top = crest[:, ROWS - 1 : ROWS]
    total = fade[0:1, ROWS - 1 : ROWS]
    mext[MD:ZR] = jnp.ones((16, ROWS), bf16)
    weighted = mext[...].astype(f32) * jnp.exp(level[0:1] - top)
    w_hi, w_lo = halves(weighted)
    z = dot(w_hi, mk_in[...]) + dot(w_lo, mk_in[...])
    zstage[0:MD] = z[0:MD].astype(bf16)
    z_rest = (
        *pieces(z[MD : MD + 1]),
        *pieces(jnp.broadcast_to(total + top, (1, MD))),
        *pieces(jnp.broadcast_to(total, (1, MD))),
    )
    zstage[MD:ZR] = rows_of(z_rest, 16, MD).astype(bf16)

    def z_copy(to):
        return pltpu.make_async_remote_copy(
            zstage, zb.at[r], z_s.at[to], z_r.at[r], device_id=(to, t), device_id_type=MESH
        )

    def z_send(to, _):
        z_copy(to).start()
        return 0

    def chunk_at(n):
        p, m = n // 4, n % 4
        pz = jnp.where(p // 2 == 1, flip(rz), rz)
        py = jnp.where(p % 2 == 1, flip(ry), ry)
        cz = jnp.where(m // 2 == 1, 3 - pz, pz)
        cy = jnp.where(m % 2 == 1, 3 - py, py)
        return 4 * cz + cy

    def sibling_uses(chunk):
        return jnp.where(b == 0, chunk <= 8 + a, chunk <= 15 - a)

    def forward_copy(chunk):
        return pltpu.make_async_remote_copy(
            kv.at[chunk, 0 : 2 * AD], kv.at[chunk, 0 : 2 * AD], f_s.at[chunk], kv_r.at[chunk],
            device_id=(r, 2 * x + 1 - k), device_id_type=MESH,
        )

    def peer_copy(chunk, n, p):
        member = jnp.where(p // 2 == 1, 2 - 2 * (a // 2), 2 * (a // 2)) + jnp.where(
            p % 2 == 1, 1 - a % 2, a % 2
        )
        return (chunk <= 15 - member), pltpu.make_async_remote_copy(
            kv.at[chunk, 0 : 2 * AD], kv.at[chunk, 0 : 2 * AD], p_s.at[n % 4, p - 1], kv_r.at[chunk],
            device_id=(chip_of(g, member), t), device_id_type=MESH,
        )

    def arrive(n, entry):
        chunk = chunk_at(n)
        mine = core_for(chunk) == b
        used = jnp.where(mine, True, jnp.where(b == 0, chunk <= 15 - a, chunk <= 8 + a))
        reaches = True if entry else chunk <= 15 - a
        own = (chunk == r) & (g // 2 == k) & mine

        @pl.when(reaches & used & jnp.logical_not(own))
        def _():
            forward_copy(chunk).wait_recv()

        @pl.when(reaches & mine)
        def _():
            for p in (1, 2, 3) if entry else ():
                wanted, copy = peer_copy(chunk, n, p)

                @pl.when(wanted)
                def _():
                    copy.start()

            @pl.when(sibling_uses(chunk))
            def _():
                forward_copy(chunk).start()

    for n in range(4):
        arrive(n, True)
    lax.fori_loop(r + 1, N_SP, z_send, 0)

    for j in range(ROWS // QT):
        cols = slice(j * QT, j * QT + QT)
        n_keys = j * QT + QT
        raw = dot(mk_in[0:n_keys], mq_in[:, cols]) * MD**-0.5
        log = levels[0:n_keys, 0:1] - crest[:, cols]
        key_at = lax.broadcasted_iota(jnp.int32, (n_keys, QT), 0)
        query_at = lax.broadcasted_iota(jnp.int32, (n_keys, QT), 1) + j * QT
        seen = key_at <= query_at
        pair = jnp.where(seen, raw * jnp.exp(jnp.where(seen, log, 0.0)), 0.0)
        p_hi, p_lo = halves(pair)
        mnum[:, cols] = dot(mext[:, 0:n_keys], p_hi) + dot(mext[:, 0:n_keys], p_lo)

    w_copies = []
    for n in range(8):
        rows = slice(n % 4 * 256, n % 4 * 256 + 256)
        src, dst = ((wa_in, wa), (wm_in, wm))[n // 4]
        w_copies.append(pltpu.make_async_copy(src.at[rows], dst.at[rows], wsem.at[n]))
        w_copies[-1].start()
    own_decay.wait()
    decay_copy().wait_recv()
    factor = scale_ref[head] * (AD**-0.5 * LOG2E)

    def decay_of(chunk):
        slab = decays[g // 2, :, pl.ds(pl.multiple_of(chunk * ROWS, ROWS), ROWS)]
        return jnp.where(g % 2 == 0, slab[0:1], slab[1:2]) * LOG2E

    for slot in range(2):
        chunk = hi if slot == 0 else lo
        own = (chunk == r) & (g // 2 == k)

        @pl.when(jnp.logical_not(own))
        def _():
            pltpu.make_async_remote_copy(
                qs.at[0], qb.at[slot], q_s.at[0], q_r.at[slot],
                device_id=(r, 2 * x + 1 - k), device_id_type=MESH,
            ).wait_recv()

        q_hi, q_mid, q_lo = pieces(qb[slot].astype(f32) * factor)
        d_hi, d_mid, d_lo = pieces(decay_of(chunk))
        qaug[slot, 0:64] = q_hi.astype(bf16)
        qaug[slot, 64:80] = rows_of((-1.0, -1.0, -1.0, d_hi, d_mid, d_lo), 16, ROWS).astype(bf16)
        qaug[slot, 80:128] = jnp.zeros((48, ROWS), bf16)
        qaug[slot, 128:192] = q_mid.astype(bf16)
        qaug[slot, 192:256] = q_lo.astype(bf16)
        best[slot] = jnp.full((8, ROWS), FAR, f32)
        acc[slot] = jnp.zeros((VEXT, ROWS), f32)

    def ones_row(chunk, _):
        kv[chunk, 2 * AD : 2 * AD + 16] = jnp.ones((16, ROWS), bf16)
        return 0

    lax.fori_loop(0, N_SP, ones_row, 0)

    def fold(slot, chunk, diag):
        def scores(i):
            n_keys = (i + 1) * QT if diag else ROWS
            s = dot(kaug[0:n_keys], qaug[slot, :, i * QT : i * QT + QT])
            if diag:
                key_at = lax.broadcasted_iota(jnp.int32, (n_keys, QT), 0)
                query_at = lax.broadcasted_iota(jnp.int32, (n_keys, QT), 1) + i * QT
                s = jnp.where(key_at <= query_at, s, FAR)
            return s

        def finish(i, s):
            cols = slice(i * QT, i * QT + QT)
            n_keys = s.shape[0]
            old = best[slot, 0:1, cols]
            new = jnp.maximum(old, jnp.max(s, axis=0, keepdims=True))
            weights = jnp.exp2(s - new).astype(bf16)
            got = dot(kv[chunk, AD : AD + VEXT, 0:n_keys], weights)
            acc[slot, :, cols] = acc[slot, :, cols] * jnp.exp2(old - new) + got
            best[slot, 0:1, cols] = new

        tiles = ROWS // QT
        s = scores(0)
        for i in range(tiles):
            later = scores(i + 1) if i + 1 < tiles else None
            finish(i, s)
            s = later

    def visit(n, _):
        @pl.when((n >= 3) & (n < 15))
        def _():
            arrive(n + 1, False)

        chunk = chunk_at(n)

        @pl.when(chunk <= hi)
        def _():
            take(chunk)

        return 0

    def take(chunk):
        keys = kv[chunk, 0:AD]
        keys32 = keys.astype(f32)
        d_hi, d_mid, d_lo = pieces(decay_of(chunk))
        extra = rows_of((d_hi, d_mid, d_lo, 1.0, 1.0, 1.0), 64, ROWS)
        kaug[:, 0:128] = jnp.concatenate([keys32, extra], axis=0).T.astype(bf16)
        kaug[:, 128:256] = jnp.concatenate([keys32, keys32], axis=0).T.astype(bf16)

        def side(slot, _):
            mine = jnp.where(slot == 0, hi, lo)

            @pl.when(chunk < mine)
            def _():
                fold(slot, chunk, False)

            @pl.when(chunk == mine)
            def _():
                fold(slot, chunk, True)

            return 0

        lax.fori_loop(0, 2, side, 0)

    lax.fori_loop(0, 16, visit, 0)

    def o_copy(slot, p):
        chunk = hi if slot == 0 else lo
        own = (chunk == r) & (p == t)
        return own, pltpu.make_async_remote_copy(
            ostage.at[slot, p], att.at[head], o_s.at[slot, p], o_r.at[head],
            device_id=(chunk, p), device_id_type=MESH,
        )

    for slot in range(2):
        result = acc[slot, 0:AD] / acc[slot, AD : AD + 1]
        result = result.astype(bf16)
        for p in range(N_TP):
            ostage[slot, p] = result[:, p * 128 : p * 128 + 128]

        def o_send(p, _):
            own, copy = o_copy(slot, p)

            @pl.when(jnp.logical_not(own))
            def _():
                copy.start()

            @pl.when(own)
            def _():
                att[head] = ostage[slot, p]

            return 0

        lax.fori_loop(0, N_TP, o_send, 0)

    z0 = jnp.concatenate(
        [cinit_in[0].T, jnp.broadcast_to(ninit_in[...], (16, MD))], axis=0
    )

    def enter(n, carry):
        state, log = carry
        pltpu.make_async_remote_copy(
            zstage, zb.at[n], z_s.at[0], z_r.at[n], device_id=(0, t), device_id_type=MESH
        ).wait_recv()
        rest = zb[n, MD:ZR].astype(f32)
        norm = rest[0:1] + rest[1:2] + rest[2:3]
        stab = rest[3:4] + rest[4:5] + rest[5:6]
        faded = log + (rest[6:7] + rest[7:8] + rest[8:9])
        new = jnp.maximum(faded, stab)
        added = jnp.concatenate(
            [zb[n, 0:MD].astype(f32), jnp.broadcast_to(norm, (16, MD))], axis=0
        )
        return state * jnp.exp(faded - new) + added * jnp.exp(stab - new), new

    state, log = lax.fori_loop(0, r, enter, (z0, jnp.zeros((1, MD), f32)))
    crest = crest_s[0:1]
    log = log[:, 0:1]
    peak = jnp.maximum(crest, log)
    s_hi, s_lo = halves(state)
    carried = (dot(s_hi, mq_in[...]) + dot(s_lo, mq_in[...])) * MD**-0.5
    numer = mnum[...] * jnp.exp(crest - peak) + carried * jnp.exp(log - peak)
    floor = jnp.exp(-(fade_s[0:1] + peak))
    recalled = numer[0:MD] / jnp.maximum(jnp.abs(numer[MD : MD + 1]), floor)
    squares = jnp.sum(recalled * recalled, axis=0, keepdims=True)
    sq_hi, sq_mid, sq_lo = pieces(squares)
    gated = (recalled * jax.nn.sigmoid(mo_in[...].astype(f32))).astype(bf16)
    stats = rows_of((sq_hi, sq_mid, sq_lo), 16, ROWS).astype(bf16)
    for p in range(N_TP):
        mstage[p, 0:MD] = gated[:, p * 128 : p * 128 + 128]
        mstage[p, MD:ZR] = stats[:, p * 128 : p * 128 + 128]

    def m_copy(p):
        return pltpu.make_async_remote_copy(
            mstage.at[p], mb.at[t], m_s.at[p], m_r.at[t], device_id=(r, p), device_id_type=MESH
        )

    def m_send(p, _):
        @pl.when(p != t)
        def _():
            m_copy(p).start()

        @pl.when(p == t)
        def _():
            mb[t] = mstage[p]

        return 0

    lax.fori_loop(0, N_TP, m_send, 0)

    def o_wait(n, _):
        own = (n == head) & ((hi == r) | (lo == r))

        @pl.when(jnp.logical_not(own))
        def _():
            pltpu.make_async_remote_copy(
                ostage.at[0, 0], att.at[n], o_s.at[0, 0], o_r.at[n],
                device_id=(r, (t + 1) % N_TP), device_id_type=MESH,
            ).wait_recv()

        return 0

    def m_wait(n, _):
        @pl.when(n != t)
        def _():
            pltpu.make_async_remote_copy(
                mstage.at[0], mb.at[n], m_s.at[0], m_r.at[n],
                device_id=(r, (t + 1) % N_TP), device_id_type=MESH,
            ).wait_recv()

        return 0

    lax.fori_loop(0, N_TP, m_wait, 0)
    for copy in w_copies:
        copy.wait()

    m_all = jnp.concatenate([mb[n, 0:MD].astype(f32).T for n in range(N_TP)], axis=1)
    m_stats = sum(mb[n, MD:ZR].astype(f32) for n in range(N_TP)).T
    m_sq = m_stats[:, 0:1] + m_stats[:, 1:2] + m_stats[:, 2:3]
    m_mix = (m_all * lax.rsqrt(m_sq / 1024.0 + EPS) * mgain_in[...]).astype(bf16)

    lax.fori_loop(0, 16, o_wait, 0)
    a_all = jnp.concatenate(
        [
            jnp.concatenate([att[2 * n], att[2 * n + 1]], axis=0).astype(f32).T
            for n in range(8)
        ],
        axis=1,
    )
    a_sq = jnp.sum(a_all * a_all, axis=1, keepdims=True)
    a_mix = (a_all * lax.rsqrt(a_sq / 1024.0 + EPS) * again_in[...]).astype(bf16)
    for n in range(4):
        cols = slice(n * 512, n * 512 + 512)
        out[:, cols] = (dot(m_mix, wm[:, cols]) + dot(a_mix, wa[:, cols])).astype(bf16)

    decay_copy().wait_send()
    for h in range(2):
        for own, copy in (q_copy(h), kv_copy(h)):

            @pl.when(jnp.logical_not(own))
            def _():
                copy.wait_send()

    def z_done(to, _):
        z_copy(to).wait_send()
        return 0

    lax.fori_loop(r + 1, N_SP, z_done, 0)

    def f_done(n, _):
        chunk = chunk_at(n)
        mine = core_for(chunk) == b
        reaches = jnp.where(n < 4, True, chunk <= 15 - a)

        @pl.when(reaches & mine)
        def _():
            @pl.when(n < 4)
            def _():
                for p in (1, 2, 3):
                    wanted, copy = peer_copy(chunk, n, p)

                    @pl.when(wanted)
                    def _():
                        copy.wait_send()

            @pl.when(sibling_uses(chunk))
            def _():
                forward_copy(chunk).wait_send()

        return 0

    lax.fori_loop(0, N_SP, f_done, 0)

    def p_done(p, _):
        for slot in range(2):
            own, copy = o_copy(slot, p)

            @pl.when(jnp.logical_not(own))
            def _():
                copy.wait_send()

        @pl.when(p != t)
        def _():
            m_copy(p).wait_send()

        return 0

    lax.fori_loop(0, N_TP, p_done, 0)


def mix(*arrays):
    smem = pl.BlockSpec(memory_space=pltpu.SMEM)
    hbm = pl.BlockSpec(memory_space=pltpu.HBM)
    dma = pltpu.SemaphoreType.DMA
    return pl.pallas_call(
        mix_kernel,
        out_shape=jax.ShapeDtypeStruct((128, 2048), bf16),
        in_specs=[smem] * 2 + [hbm] * 18,
        out_specs=pl.BlockSpec(memory_space=pltpu.VMEM),
        scratch_shapes=[
            pltpu.VMEM((ROWS, 2048), bf16),
            pltpu.VMEM((2048, 1024), bf16),
            pltpu.VMEM((8, 2048), bf16),
            pltpu.VMEM((1, 2048), f32),
            pltpu.VMEM((1, ROWS), f32),
            pltpu.VMEM((1, MD, MD), f32),
            pltpu.VMEM((1, MD), f32),
            pltpu.VMEM((1, 1024), f32),
            pltpu.VMEM((1, 1024), f32),
            pltpu.VMEM((2, AD, ROWS), bf16),
            pltpu.VMEM((2, 2 * AD, ROWS), bf16),
            pltpu.VMEM((MD, ROWS), bf16),
            pltpu.VMEM((ROWS, MD), bf16),
            pltpu.VMEM((MD, ROWS), bf16),
            pltpu.VMEM((8, ROWS), f32),
            pltpu.VMEM((8, ROWS), f32),
            pltpu.VMEM((ROWS, 8), f32),
            pltpu.VMEM((1024, 2048), bf16),
            pltpu.VMEM((1024, 2048), bf16),
            pltpu.VMEM((N_SP, 2 * AD + 16, ROWS), bf16),
            pltpu.VMEM((2, AD, ROWS), bf16),
            pltpu.VMEM((2, 2, N_SP * ROWS), f32),
            pltpu.VMEM((ROWS, 256), bf16),
            pltpu.VMEM((2, 256, ROWS), bf16),
            pltpu.VMEM((2, 8, ROWS), f32),
            pltpu.VMEM((2, VEXT, ROWS), f32),
            pltpu.VMEM((2, N_TP, AD, 128), bf16),
            pltpu.VMEM((16, AD, 128), bf16),
            pltpu.VMEM((ZR, MD), bf16),
            pltpu.VMEM((N_SP, ZR, MD), bf16),
            pltpu.VMEM((N_TP, ZR, 128), bf16),
            pltpu.VMEM((N_TP, ZR, 128), bf16),
            pltpu.VMEM((ZR, ROWS), bf16),
            pltpu.VMEM((ZR, ROWS), f32),
            dma((20,)), dma((8,)),
            dma((2,)), dma((N_SP,)),
            dma((2,)), dma((2,)),
            dma((N_SP,)), dma((N_SP,)),
            dma((N_TP,)), dma((N_TP,)),
            dma((2, N_TP)), dma((16,)),
            dma((4, 3)), dma((N_SP,)), dma, dma,
        ],
        compiler_params=pltpu.CompilerParams(
            collective_id=0, has_side_effects=True, vmem_limit_bytes=60 * 2**20
        ),
        cost_estimate=pl.CostEstimate(
            flops=60 * 10**9, bytes_accessed=12 * 2**20, transcendentals=0
        ),
    )(*arrays)


def on_device(tokens, norm_gain, attn_query, attn_key, attn_value, score_scale, attention_decay,
              mem_query, mem_key, mem_value, mem_ingate, input_shift, memory_decay, mem_outgate,
              init_memory, init_normalizer, attn_gain, mem_gain, attn_out, mem_out):
    return mix(
        score_scale, input_shift, tokens, attn_query, attn_key, attn_value, mem_query, mem_key,
        mem_value, mem_outgate, mem_ingate.T, norm_gain.reshape(1, 2048), memory_decay,
        attention_decay, init_memory, init_normalizer, attn_gain.reshape(1, 1024),
        mem_gain.reshape(1, 1024), attn_out, mem_out,
    )


def solution(mesh):
    tp = P(None, "tp")
    placed = (
        P("sp", None), P(), tp, tp, tp, P(), P("tp", None), tp, tp, tp, P(), P(),
        P("tp", "sp"), tp, P("tp", None, None), P("tp", None), P(), P(), P(), P(),
    )
    return jax.shard_map(
        on_device, mesh=mesh, in_specs=placed, out_specs=P(("sp", "tp"), None), check_vma=False
    )
```

```python
import functools
import math

import jax
import jax.numpy as jnp
from jax import lax
from jax.experimental import pallas as pl
from jax.experimental.pallas import tpu as pltpu
from jax.sharding import PartitionSpec as P

MESH = pl.DeviceIdType.MESH
f32 = jnp.float32
bf16 = jnp.bfloat16
EPS = 1e-06
LOG2E = math.log2(math.e)
FAR = -1e30
ROWS = 1024
AD = 64
MD = 128
QT = 256
N_SP, N_TP = 16, 8
RECALL_AT = 12
VEXT = AD + 16
ZR = MD + 16


def dot(a, b):
    return jnp.dot(a, b, preferred_element_type=f32)


def pieces(x):
    hi = x.astype(bf16).astype(f32)
    rest = x - hi
    mid = rest.astype(bf16).astype(f32)
    low = (rest - mid).astype(bf16).astype(f32)
    return hi, mid, low


def halves(x):
    hi = x.astype(bf16)
    return hi, (x - hi.astype(f32)).astype(bf16)


def rows_of(values, height, width):
    at = lax.broadcasted_iota(jnp.int32, (height, width), 0)
    out = jnp.zeros((height, width), f32)
    for n, value in enumerate(values):
        out = jnp.where(at == n, value, out)
    return out


def shifted(x, by, fill):
    at = lax.broadcasted_iota(jnp.int32, x.shape, 1)
    return jnp.where(at >= by, pltpu.roll(x, by, 1), fill)


def scan_lanes(x, join, fill):
    by = 1
    while by < x.shape[1]:
        x = join(x, shifted(x, by, fill))
        by *= 2
    return x


def mix_kernel(scale_ref, shift_ref, tok_in, wq_in, wk_in, wv_in, wmq_in, wmk_in, wmv_in, wmo_in, ing_in,
               ngain_in, fade_hbm, decay_in, cinit_hbm, ninit_hbm, again_hbm, mgain_hbm, wa_in, wm_in,
               out, tok, w, ing, ngain, fade_in, cinit_in, ninit_in, again_in, mgain_in,
               qs, kvs, mq_in, mk_in, mo_in, fade_s, crest_s, levels,
               wa, wm, kv, qb, decays, kaug, qaug, best, acc, ostage, att,
               zstage, zb, mstage, mb, mext, mnum, half,
               isem, wsem, kv_s, kv_r, q_s, q_r, z_s, z_r, m_s, m_r, o_s, o_r, p_s, f_s, d_s, d_r):
    r = lax.axis_index("sp")
    t = lax.axis_index("tp")
    x, k = t // 2, t % 2
    rz, ry = r // 4, r % 4

    def member(z, y):
        m = 2 * (z % 2) + y % 2
        return jnp.where(z // 2 == 1, 3 - m, m)

    g = 2 * (rz // 2) + ry // 2
    a = member(rz, ry)
    b = k
    hi = jnp.where(b == 0, 15 - a, 8 + a)
    lo = jnp.where(b == 0, a, 7 - a)
    head = 4 * x + g

    def chip_of(block, member):
        m = jnp.where(block // 2 == 1, 3 - member, member)
        return 4 * (2 * (block // 2) + m // 2) + 2 * (block % 2) + m % 2

    def flip(v):
        return v + 1 - 2 * (v % 2)

    def core_for(chunk):
        return (chunk % 4) // 2

    loads = []

    def load(src, dst):
        copy = pltpu.make_async_copy(src, dst, isem.at[len(loads)])
        copy.start()
        loads.append(copy)
        return copy

    small = [
        load(ngain_in, ngain), load(ing_in, ing), load(fade_hbm, fade_in), load(cinit_hbm, cinit_in),
        load(ninit_hbm, ninit_in), load(again_hbm, again_in), load(mgain_hbm, mgain_in),
    ]
    tok_loads = []
    first = []
    rest = []
    for i in range(4):
        rows = slice(i * 256, i * 256 + 256)
        tok_loads.append(load(tok_in.at[rows], tok.at[rows]))
        if i == 0:
            for n, ref in ((0, wq_in), (1, wk_in), (2, wv_in), (3, wmk_in)):
                first.append(load(ref, w.at[:, n * 128 : n * 128 + 128]))
    for n, ref in ((4, wmq_in), (5, wmv_in), (6, wmo_in)):
        rest.append(load(ref, w.at[:, n * 128 : n * 128 + 128]))
    own_decay = load(decay_in, decays.at[k])

    barrier = pltpu.get_barrier_semaphore()
    me = r * N_TP + t

    def greet(n, _):
        other = (me + n) % (N_SP * N_TP)
        pl.semaphore_signal(
            barrier, inc=1, device_id=(other // N_TP, other % N_TP), device_id_type=MESH
        )
        return 0

    lax.fori_loop(1, N_SP * N_TP, greet, 0)

    for copy in small:
        copy.wait()
    for copy in first:
        copy.wait()

    def unit(v):
        return (v * lax.rsqrt(jnp.mean(v * v, axis=0, keepdims=True) + EPS)).astype(bf16)

    def turned(p):
        return p.astype(bf16).astype(f32).T

    for i in range(4):
        rows = slice(i * 256, i * 256 + 256)
        tok_loads[i].wait()
        v = tok[rows].astype(f32)
        ms = jnp.mean(v * v, axis=-1, keepdims=True)
        n = (v * lax.rsqrt(ms + EPS) * ngain[...]).astype(bf16)
        tok[rows] = n
        p = dot(n, w[:, 0:256])
        pq, pk = turned(p[:, :128]), turned(p[:, 128:])
        for h in range(2):
            qs[h, :, rows] = unit(pq[h * AD : h * AD + AD])
            kvs[h, 0:AD, rows] = unit(pk[h * AD : h * AD + AD])
        p = dot(n, w[:, 256:512])
        pv = turned(p[:, :128]).astype(bf16)
        for h in range(2):
            kvs[h, AD : 2 * AD, rows] = pv[h * AD : h * AD + AD]
        mk_in[rows] = p[:, 128:].astype(bf16)

    pl.semaphore_wait(barrier, N_SP * N_TP - 1)

    def worker(chunk):
        quarter, low = chunk // 4, chunk % 4
        wa_ = jnp.where(quarter % 2 == 0, low, 3 - low)
        wb = jnp.where((quarter == 0) | (quarter == 3), 0, 1)
        slot = jnp.where(quarter >= 2, 0, 1)
        return wa_, wb, slot

    my_a, my_b, my_slot = worker(r)

    def q_copy(h):
        sp, tp = chip_of(2 * k + h, my_a), 2 * x + my_b
        own = (sp == r) & (tp == t)
        return own, pltpu.make_async_remote_copy(
            qs.at[h], qb.at[my_slot], q_s.at[h], q_r.at[my_slot],
            device_id=(sp, tp), device_id_type=MESH,
        )

    def kv_copy(h):
        block = 2 * k + h
        z = jnp.where(rz // 2 == block // 2, rz, 3 - rz)
        y = jnp.where(ry // 2 == block % 2, ry, 3 - ry)
        sp, tp = 4 * z + y, 2 * x + core_for(r)
        own = (sp == r) & (tp == t)
        return own, pltpu.make_async_remote_copy(
            kvs.at[h], kv.at[r, 0 : 2 * AD], kv_s.at[h], kv_r.at[r],
            device_id=(sp, tp), device_id_type=MESH,
        )

    def decay_copy():
        return pltpu.make_async_remote_copy(
            decay_in, decays.at[k], d_s, d_r, device_id=(r, 2 * x + 1 - k), device_id_type=MESH
        )

    decay_copy().start()
    for h in range(2):
        own, copy = q_copy(h)

        @pl.when(jnp.logical_not(own))
        def _():
            copy.start()

        @pl.when(own)
        def _():
            qb[my_slot] = qs[h]

    for h in range(2):
        own, copy = kv_copy(h)

        @pl.when(jnp.logical_not(own))
        def _():
            copy.start()

        @pl.when(own)
        def _():
            kv[r, 0 : 2 * AD] = kvs[h]

    def peer(p):
        z = flip(rz) if p // 2 else rz
        y = flip(ry) if p % 2 else ry
        return 4 * z + y, member(z, y)

    def block_copy(p):
        chip, its_a = peer(p)
        wanted = (g // 2 == k) & (r <= 15 - its_a)
        return wanted, pltpu.make_async_remote_copy(
            kvs.at[g % 2], kv.at[r, 0 : 2 * AD], p_s.at[0, p - 1], kv_r.at[r],
            device_id=(chip, 2 * x + core_for(r)), device_id_type=MESH,
        )

    for p in (1, 2, 3):
        wanted, copy = block_copy(p)

        @pl.when(wanted)
        def _():
            copy.start()

    w[:, 896:1024] = jnp.zeros((2048, 128), bf16)
    w[:, 896:904] = ing[...].astype(f32).T.astype(bf16)
    for copy in rest:
        copy.wait()
    gates = []
    for i in range(4):
        rows = slice(i * 256, i * 256 + 256)
        p = dot(tok[rows], w[:, 512:768])
        mq_in[:, rows] = turned(p[:, :128]).astype(bf16)
        mext[0:MD, rows] = turned(p[:, 128:]).astype(bf16)
        p = dot(tok[rows], w[:, 768:1024])
        mo_in[:, rows] = turned(p[:, :128]).astype(bf16)
        gates.append(p[:, 128:].T[0:8])

    gate8 = jnp.concatenate(gates, axis=1)
    gate = jnp.sum(
        jnp.where(lax.broadcasted_iota(jnp.int32, (8, ROWS), 0) == t, gate8, 0.0),
        axis=0, keepdims=True,
    ) + shift_ref[t]
    fade = scan_lanes(jnp.broadcast_to(fade_in[...], (8, ROWS)), jnp.add, 0.0)
    level = jnp.broadcast_to(gate, (8, ROWS)) - fade
    crest8 = scan_lanes(level, jnp.maximum, FAR)
    fade_s[...] = fade
    crest_s[...] = crest8
    levels[...] = level.T
    crest = crest8[0:1]
    top = crest[:, ROWS - 1 : ROWS]
    total = fade[0:1, ROWS - 1 : ROWS]
    mext[MD:ZR] = jnp.ones((16, ROWS), bf16)
    weighted = mext[...].astype(f32) * jnp.exp(level[0:1] - top)
    w_hi, w_lo = halves(weighted)
    z = dot(w_hi, mk_in[...]) + dot(w_lo, mk_in[...])
    zstage[0:MD] = z[0:MD].astype(bf16)
    z_rest = (
        *pieces(z[MD : MD + 1]),
        *pieces(jnp.broadcast_to(total + top, (1, MD))),
        *pieces(jnp.broadcast_to(total, (1, MD))),
    )
    zstage[MD:ZR] = rows_of(z_rest, 16, MD).astype(bf16)

    def z_copy(to):
        return pltpu.make_async_remote_copy(
            zstage, zb.at[r], z_s.at[to], z_r.at[r], device_id=(to, t), device_id_type=MESH
        )

    def z_send(to, _):
        z_copy(to).start()
        return 0

    def chunk_at(n):
        p = jnp.where(
            n < 4, 0, jnp.where(n < 7, n - 3, jnp.where(n < 13, (n - 5) // 2, n - 12))
        )
        m = jnp.where(n < 4, n, jnp.where(n < 7, 0, jnp.where(n < 13, 1 + (n - 7) % 2, 3)))
        pz = jnp.where(p // 2 == 1, flip(rz), rz)
        py = jnp.where(p % 2 == 1, flip(ry), ry)
        cz = jnp.where(m // 2 == 1, 3 - pz, pz)
        cy = jnp.where(m % 2 == 1, 3 - py, py)
        return 4 * cz + cy

    def sibling_uses(chunk):
        return jnp.where(b == 0, chunk <= 8 + a, chunk <= 15 - a)

    def forward_copy(chunk):
        return pltpu.make_async_remote_copy(
            kv.at[chunk, 0 : 2 * AD], kv.at[chunk, 0 : 2 * AD], f_s.at[chunk], kv_r.at[chunk],
            device_id=(r, 2 * x + 1 - k), device_id_type=MESH,
        )

    def peer_copy(chunk, n, p):
        chip, its_a = peer(p)
        return (chunk <= 15 - its_a), pltpu.make_async_remote_copy(
            kv.at[chunk, 0 : 2 * AD], kv.at[chunk, 0 : 2 * AD], p_s.at[n % 4, p - 1], kv_r.at[chunk],
            device_id=(chip, t), device_id_type=MESH,
        )

    def arrive(n, entry):
        chunk = chunk_at(n)
        mine = core_for(chunk) == b
        used = jnp.where(mine, True, jnp.where(b == 0, chunk <= 15 - a, chunk <= 8 + a))
        reaches = True if entry else chunk <= 15 - a
        own = (chunk == r) & (g // 2 == k) & mine

        @pl.when(reaches & used & jnp.logical_not(own))
        def _():
            forward_copy(chunk).wait_recv()

        @pl.when(reaches & mine)
        def _():
            for p in (1, 2, 3) if entry and n > 0 else ():
                wanted, copy = peer_copy(chunk, n, p)

                @pl.when(wanted)
                def _():
                    copy.start()

            @pl.when(sibling_uses(chunk))
            def _():
                forward_copy(chunk).start()

    for j in range(ROWS // QT):
        cols = slice(j * QT, j * QT + QT)
        n_keys = j * QT + QT
        raw = dot(mk_in[0:n_keys], mq_in[:, cols]) * MD**-0.5
        log = levels[0:n_keys, 0:1] - crest[:, cols]
        key_at = lax.broadcasted_iota(jnp.int32, (n_keys, QT), 0)
        query_at = lax.broadcasted_iota(jnp.int32, (n_keys, QT), 1) + j * QT
        seen = key_at <= query_at
        pair = jnp.where(seen, raw * jnp.exp(jnp.where(seen, log, 0.0)), 0.0)
        p_hi, p_lo = halves(pair)
        mnum[:, cols] = dot(mext[:, 0:n_keys], p_hi) + dot(mext[:, 0:n_keys], p_lo)

    arrive(0, True)

    w_copies = []
    for n in range(8):
        rows = slice(n % 4 * 256, n % 4 * 256 + 256)
        src, dst = ((wa_in, wa), (wm_in, wm))[n // 4]
        w_copies.append(pltpu.make_async_copy(src.at[rows], dst.at[rows], wsem.at[n]))
        w_copies[-1].start()
    own_decay.wait()
    decay_copy().wait_recv()
    factor = scale_ref[head] * (AD**-0.5 * LOG2E)

    def decay_of(chunk):
        slab = decays[g // 2, :, pl.ds(pl.multiple_of(chunk * ROWS, ROWS), ROWS)]
        return jnp.where(g % 2 == 0, slab[0:1], slab[1:2]) * LOG2E

    for slot in range(2):
        chunk = hi if slot == 0 else lo
        own = (chunk == r) & (g // 2 == k)

        @pl.when(jnp.logical_not(own))
        def _():
            pltpu.make_async_remote_copy(
                qs.at[0], qb.at[slot], q_s.at[0], q_r.at[slot],
                device_id=(r, 2 * x + 1 - k), device_id_type=MESH,
            ).wait_recv()

        q_hi, q_mid, q_lo = pieces(qb[slot].astype(f32) * factor)
        d_hi, d_mid, d_lo = pieces(decay_of(chunk))
        qaug[slot, 0:64] = q_hi.astype(bf16)
        qaug[slot, 64:80] = rows_of((-1.0, -1.0, -1.0, d_hi, d_mid, d_lo), 16, ROWS).astype(bf16)
        qaug[slot, 80:128] = jnp.zeros((48, ROWS), bf16)
        qaug[slot, 128:192] = q_mid.astype(bf16)
        qaug[slot, 192:256] = q_lo.astype(bf16)
        best[slot] = jnp.full((8, ROWS), FAR, f32)
        acc[slot] = jnp.zeros((VEXT, ROWS), f32)

    def ones_row(chunk, _):
        kv[chunk, 2 * AD : 2 * AD + 16] = jnp.ones((16, ROWS), bf16)
        return 0

    lax.fori_loop(0, N_SP, ones_row, 0)

    def fold(slot, chunk, diag):
        def scores(i):
            cols = slice(i * QT, i * QT + QT)
            out = []
            for j in range(i + 1 if diag else ROWS // QT):
                s = dot(kaug[j * QT : j * QT + QT], qaug[slot, :, cols])
                if diag and j == i:
                    key_at = lax.broadcasted_iota(jnp.int32, (QT, QT), 0)
                    query_at = lax.broadcasted_iota(jnp.int32, (QT, QT), 1)
                    s = jnp.where(key_at <= query_at, s, FAR)
                out.append(s)
            return out

        def finish(i, parts):
            cols = slice(i * QT, i * QT + QT)
            old = best[slot, 0:1, cols]
            tops = parts[0]
            for s in parts[1:]:
                tops = jnp.maximum(tops, s)
            new = jnp.maximum(old, jnp.max(tops, axis=0, keepdims=True))
            got = jnp.zeros((VEXT, QT), f32)
            for j, s in enumerate(parts):
                weights = jnp.exp2(s - new).astype(bf16)
                got = got + dot(kv[chunk, AD : AD + VEXT, j * QT : j * QT + QT], weights)
            acc[slot, :, cols] = acc[slot, :, cols] * jnp.exp2(old - new) + got
            best[slot, 0:1, cols] = new

        tiles = ROWS // QT
        s = scores(0)
        for i in range(tiles):
            later = scores(i + 1) if i + 1 < tiles else None
            finish(i, s)
            s = later

    def m_copy(p):
        return pltpu.make_async_remote_copy(
            mstage.at[p], mb.at[t], m_s.at[p], m_r.at[t], device_id=(r, p), device_id_type=MESH
        )

    def m_send(p, _):
        @pl.when(p != t)
        def _():
            m_copy(p).start()

        @pl.when(p == t)
        def _():
            mb[t] = mstage[p]

        return 0

    def recall():
        z0 = jnp.concatenate(
            [cinit_in[0].T, jnp.broadcast_to(ninit_in[...], (16, MD))], axis=0
        )

        def enter(n, carry):
            state, log = carry
            pltpu.make_async_remote_copy(
                zstage, zb.at[n], z_s.at[0], z_r.at[n], device_id=(0, t), device_id_type=MESH
            ).wait_recv()
            rest = zb[n, MD:ZR].astype(f32)
            norm = rest[0:1] + rest[1:2] + rest[2:3]
            stab = rest[3:4] + rest[4:5] + rest[5:6]
            faded = log + (rest[6:7] + rest[7:8] + rest[8:9])
            new = jnp.maximum(faded, stab)
            added = jnp.concatenate(
                [zb[n, 0:MD].astype(f32), jnp.broadcast_to(norm, (16, MD))], axis=0
            )
            return state * jnp.exp(faded - new) + added * jnp.exp(stab - new), new

        state, log = lax.fori_loop(0, r, enter, (z0, jnp.zeros((1, MD), f32)))
        crest = crest_s[0:1]
        log = log[:, 0:1]
        peak = jnp.maximum(crest, log)
        s_hi, s_lo = halves(state)
        carried = (dot(s_hi, mq_in[...]) + dot(s_lo, mq_in[...])) * MD**-0.5
        numer = mnum[...] * jnp.exp(crest - peak) + carried * jnp.exp(log - peak)
        floor = jnp.exp(-(fade_s[0:1] + peak))
        recalled = numer[0:MD] / jnp.maximum(jnp.abs(numer[MD : MD + 1]), floor)
        squares = jnp.sum(recalled * recalled, axis=0, keepdims=True)
        sq_hi, sq_mid, sq_lo = pieces(squares)
        gated = (recalled * jax.nn.sigmoid(mo_in[...].astype(f32))).astype(bf16)
        stats = rows_of((sq_hi, sq_mid, sq_lo), 16, ROWS).astype(bf16)
        for p in range(N_TP):
            mstage[p, 0:MD] = gated[:, p * 128 : p * 128 + 128]
            mstage[p, MD:ZR] = stats[:, p * 128 : p * 128 + 128]

        lax.fori_loop(0, N_TP, m_send, 0)

    def o_copy(slot, p):
        chunk = hi if slot == 0 else lo
        own = (chunk == r) & (p == t)
        return own, pltpu.make_async_remote_copy(
            ostage.at[slot, p], att.at[head], o_s.at[slot, p], o_r.at[head],
            device_id=(chunk, p), device_id_type=MESH,
        )

    def depart(slot):
        result = acc[slot, 0:AD] / acc[slot, AD : AD + 1]
        result = result.astype(bf16)
        for p in range(N_TP):
            ostage[slot, p] = result[:, p * 128 : p * 128 + 128]

        def o_send(p, _):
            own, copy = o_copy(slot, p)

            @pl.when(jnp.logical_not(own))
            def _():
                copy.start()

            @pl.when(own)
            def _():
                att[head] = ostage[slot, p]

            return 0

        lax.fori_loop(0, N_TP, o_send, 0)

    def visit(n, early):
        @pl.when((n >= 3) & (n < 15))
        def _():
            arrive(n + 1, False)

        chunk = chunk_at(n)

        @pl.when(chunk <= hi)
        def _():
            take(chunk)

        early = early + jnp.where(chunk <= lo, 1, 0)

        @pl.when((chunk <= lo) & (early == lo + 1))
        def _():
            depart(1)

        @pl.when(n == 0)
        def _():
            arrive(1, True)
            arrive(2, True)

        @pl.when(n == 1)
        def _():
            arrive(3, True)
            lax.fori_loop(r + 1, N_SP, z_send, 0)

        @pl.when(n == RECALL_AT)
        def _():
            recall()

        return early

    def take(chunk):
        keys = kv[chunk, 0:AD]
        d_hi, d_mid, d_lo = pieces(decay_of(chunk))
        extra = rows_of((d_hi, d_mid, d_lo, 1.0, 1.0, 1.0), 64, ROWS)
        kaug[:, 0:128] = jnp.concatenate([keys, extra.astype(bf16)], axis=0).T
        kaug[:, 128:256] = jnp.concatenate([keys, keys], axis=0).T

        def side(slot, _):
            mine = jnp.where(slot == 0, hi, lo)

            @pl.when(chunk < mine)
            def _():
                fold(slot, chunk, False)

            @pl.when(chunk == mine)
            def _():
                fold(slot, chunk, True)

            return 0

        lax.fori_loop(0, 2, side, 0)

    lax.fori_loop(0, 16, visit, 0)

    depart(0)

    def o_wait(n, _):
        own = (n == head) & ((hi == r) | (lo == r))

        @pl.when(jnp.logical_not(own))
        def _():
            pltpu.make_async_remote_copy(
                ostage.at[0, 0], att.at[n], o_s.at[0, 0], o_r.at[n],
                device_id=(r, (t + 1) % N_TP), device_id_type=MESH,
            ).wait_recv()

        return 0

    def m_wait(n, _):
        @pl.when(n != t)
        def _():
            pltpu.make_async_remote_copy(
                mstage.at[0], mb.at[n], m_s.at[0], m_r.at[n],
                device_id=(r, (t + 1) % N_TP), device_id_type=MESH,
            ).wait_recv()

        return 0

    lax.fori_loop(0, N_TP, m_wait, 0)
    for copy in w_copies:
        copy.wait()

    m_all = jnp.concatenate([mb[n, 0:MD].astype(f32).T for n in range(N_TP)], axis=1)
    m_stats = sum(mb[n, MD:ZR].astype(f32) for n in range(N_TP)).T
    m_sq = m_stats[:, 0:1] + m_stats[:, 1:2] + m_stats[:, 2:3]
    m_mix = (m_all * lax.rsqrt(m_sq / 1024.0 + EPS) * mgain_in[...]).astype(bf16)

    for n in range(4):
        cols = slice(n * 512, n * 512 + 512)
        half[:, cols] = dot(m_mix, wm[:, cols])

    decay_copy().wait_send()
    for h in range(2):
        for own, copy in (q_copy(h), kv_copy(h)):

            @pl.when(jnp.logical_not(own))
            def _():
                copy.wait_send()

    for p in (1, 2, 3):
        wanted, copy = block_copy(p)

        @pl.when(wanted)
        def _():
            copy.wait_send()

    def z_done(to, _):
        z_copy(to).wait_send()
        return 0

    lax.fori_loop(r + 1, N_SP, z_done, 0)

    def f_done(n, _):
        chunk = chunk_at(n)
        mine = core_for(chunk) == b
        reaches = jnp.where(n < 4, True, chunk <= 15 - a)

        @pl.when(reaches & mine)
        def _():
            @pl.when((n > 0) & (n < 4))
            def _():
                for p in (1, 2, 3):
                    wanted, copy = peer_copy(chunk, n, p)

                    @pl.when(wanted)
                    def _():
                        copy.wait_send()

            @pl.when(sibling_uses(chunk))
            def _():
                forward_copy(chunk).wait_send()

        return 0

    lax.fori_loop(0, N_SP, f_done, 0)

    lax.fori_loop(0, 16, o_wait, 0)
    a_all = jnp.concatenate(
        [
            jnp.concatenate([att[2 * n], att[2 * n + 1]], axis=0).astype(f32).T
            for n in range(8)
        ],
        axis=1,
    )
    a_sq = jnp.sum(a_all * a_all, axis=1, keepdims=True)
    a_mix = (a_all * lax.rsqrt(a_sq / 1024.0 + EPS) * again_in[...]).astype(bf16)
    for n in range(4):
        cols = slice(n * 512, n * 512 + 512)
        out[:, cols] = (half[:, cols] + dot(a_mix, wa[:, cols])).astype(bf16)

    def p_done(p, _):
        for slot in range(2):
            own, copy = o_copy(slot, p)

            @pl.when(jnp.logical_not(own))
            def _():
                copy.wait_send()

        @pl.when(p != t)
        def _():
            m_copy(p).wait_send()

        return 0

    lax.fori_loop(0, N_TP, p_done, 0)


def mix(*arrays):
    smem = pl.BlockSpec(memory_space=pltpu.SMEM)
    hbm = pl.BlockSpec(memory_space=pltpu.HBM)
    dma = pltpu.SemaphoreType.DMA
    return pl.pallas_call(
        mix_kernel,
        out_shape=jax.ShapeDtypeStruct((128, 2048), bf16),
        in_specs=[smem] * 2 + [hbm] * 18,
        out_specs=pl.BlockSpec(memory_space=pltpu.VMEM),
        scratch_shapes=[
            pltpu.VMEM((ROWS, 2048), bf16),
            pltpu.VMEM((2048, 1024), bf16),
            pltpu.VMEM((8, 2048), bf16),
            pltpu.VMEM((1, 2048), f32),
            pltpu.VMEM((1, ROWS), f32),
            pltpu.VMEM((1, MD, MD), f32),
            pltpu.VMEM((1, MD), f32),
            pltpu.VMEM((1, 1024), f32),
            pltpu.VMEM((1, 1024), f32),
            pltpu.VMEM((2, AD, ROWS), bf16),
            pltpu.VMEM((2, 2 * AD, ROWS), bf16),
            pltpu.VMEM((MD, ROWS), bf16),
            pltpu.VMEM((ROWS, MD), bf16),
            pltpu.VMEM((MD, ROWS), bf16),
            pltpu.VMEM((8, ROWS), f32),
            pltpu.VMEM((8, ROWS), f32),
            pltpu.VMEM((ROWS, 8), f32),
            pltpu.VMEM((1024, 2048), bf16),
            pltpu.VMEM((1024, 2048), bf16),
            pltpu.VMEM((N_SP, 2 * AD + 16, ROWS), bf16),
            pltpu.VMEM((2, AD, ROWS), bf16),
            pltpu.VMEM((2, 2, N_SP * ROWS), f32),
            pltpu.VMEM((ROWS, 256), bf16),
            pltpu.VMEM((2, 256, ROWS), bf16),
            pltpu.VMEM((2, 8, ROWS), f32),
            pltpu.VMEM((2, VEXT, ROWS), f32),
            pltpu.VMEM((2, N_TP, AD, 128), bf16),
            pltpu.VMEM((16, AD, 128), bf16),
            pltpu.VMEM((ZR, MD), bf16),
            pltpu.VMEM((N_SP, ZR, MD), bf16),
            pltpu.VMEM((N_TP, ZR, 128), bf16),
            pltpu.VMEM((N_TP, ZR, 128), bf16),
            pltpu.VMEM((ZR, ROWS), bf16),
            pltpu.VMEM((ZR, ROWS), f32),
            pltpu.VMEM((128, 2048), f32),
            dma((20,)), dma((8,)),
            dma((2,)), dma((N_SP,)),
            dma((2,)), dma((2,)),
            dma((N_SP,)), dma((N_SP,)),
            dma((N_TP,)), dma((N_TP,)),
            dma((2, N_TP)), dma((16,)),
            dma((4, 3)), dma((N_SP,)), dma, dma,
        ],
        compiler_params=pltpu.CompilerParams(
            collective_id=0, has_side_effects=True, vmem_limit_bytes=60 * 2**20
        ),
        cost_estimate=pl.CostEstimate(
            flops=60 * 10**9, bytes_accessed=12 * 2**20, transcendentals=0
        ),
    )(*arrays)


def on_device(tokens, norm_gain, attn_query, attn_key, attn_value, score_scale, attention_decay,
              mem_query, mem_key, mem_value, mem_ingate, input_shift, memory_decay, mem_outgate,
              init_memory, init_normalizer, attn_gain, mem_gain, attn_out, mem_out):
    return mix(
        score_scale, input_shift, tokens, attn_query, attn_key, attn_value, mem_query, mem_key,
        mem_value, mem_outgate, mem_ingate.T, norm_gain.reshape(1, 2048), memory_decay,
        attention_decay, init_memory, init_normalizer, attn_gain.reshape(1, 1024),
        mem_gain.reshape(1, 1024), attn_out, mem_out,
    )


def solution(mesh):
    tp = P(None, "tp")
    placed = (
        P("sp", None), P(), tp, tp, tp, P(), P("tp", None), tp, tp, tp, P(), P(),
        P("tp", "sp"), tp, P("tp", None, None), P("tp", None), P(), P(), P(), P(),
    )
    return jax.shard_map(
        on_device, mesh=mesh, in_specs=placed, out_specs=P(("sp", "tp"), None), check_vma=False
    )
```

```python
import functools
import math

import jax
import jax.numpy as jnp
from jax import lax
from jax.experimental import pallas as pl
from jax.experimental.pallas import tpu as pltpu
from jax.sharding import PartitionSpec as P

MESH = pl.DeviceIdType.MESH
f32 = jnp.float32
bf16 = jnp.bfloat16
EPS = 1e-06
LOG2E = math.log2(math.e)
FAR = -1e30
ROWS = 1024
AD = 64
MD = 128
QT = 256
N_SP, N_TP = 16, 8
ROW_AT = 7
RECALL_AT = 12
VEXT = AD + 16
ZR = MD + 16


def dot(a, b):
    return jnp.dot(a, b, preferred_element_type=f32)


def pieces(x):
    hi = x.astype(bf16).astype(f32)
    rest = x - hi
    mid = rest.astype(bf16).astype(f32)
    low = (rest - mid).astype(bf16).astype(f32)
    return hi, mid, low


def halves(x):
    hi = x.astype(bf16)
    return hi, (x - hi.astype(f32)).astype(bf16)


def rows_of(values, height, width):
    at = lax.broadcasted_iota(jnp.int32, (height, width), 0)
    out = jnp.zeros((height, width), f32)
    for n, value in enumerate(values):
        out = jnp.where(at == n, value, out)
    return out


def shifted(x, by, fill):
    at = lax.broadcasted_iota(jnp.int32, x.shape, 1)
    return jnp.where(at >= by, pltpu.roll(x, by, 1), fill)


def scan_lanes(x, join, fill):
    by = 1
    while by < x.shape[1]:
        x = join(x, shifted(x, by, fill))
        by *= 2
    return x


def mix_kernel(scale_ref, shift_ref, tok_in, wq_in, wk_in, wv_in, wmq_in, wmk_in, wmv_in, wmo_in, ing_in,
               ngain_in, fade_hbm, decay_in, cinit_hbm, ninit_hbm, again_hbm, mgain_hbm, wa_in, wm_in,
               out, tok, w, ing, ngain, fade_in, cinit_in, ninit_in, again_in, mgain_in,
               qs, kvs, mq_in, mk_in, mo_in, fade_s, crest_s, levels,
               wa, wm, kv, qb, decays, kaug, qaug, best, acc, ostage, att,
               zstage, zb, rowstage, rowb, mstage, mb, mext, mnum, half,
               isem, wsem, kv_s, kv_r, q_s, q_r, z_s, z_r, row_s, row_r, m_s, m_r, o_s, o_r, p_s, f_s, d_s, d_r):
    r = lax.axis_index("sp")
    t = lax.axis_index("tp")
    x, k = t // 2, t % 2
    rz, ry = r // 4, r % 4

    def member(z, y):
        m = 2 * (z % 2) + y % 2
        return jnp.where(z // 2 == 1, 3 - m, m)

    g = 2 * (rz // 2) + ry // 2
    a = member(rz, ry)
    b = k
    hi = jnp.where(b == 0, 15 - a, 8 + a)
    lo = jnp.where(b == 0, a, 7 - a)
    head = 4 * x + g

    def chip_of(block, member):
        m = jnp.where(block // 2 == 1, 3 - member, member)
        return 4 * (2 * (block // 2) + m // 2) + 2 * (block % 2) + m % 2

    def flip(v):
        return v + 1 - 2 * (v % 2)

    def core_for(chunk):
        return (chunk % 4) // 2

    loads = []

    def load(src, dst):
        copy = pltpu.make_async_copy(src, dst, isem.at[len(loads)])
        copy.start()
        loads.append(copy)
        return copy

    small = [
        load(ngain_in, ngain), load(ing_in, ing), load(fade_hbm, fade_in), load(cinit_hbm, cinit_in),
        load(ninit_hbm, ninit_in), load(again_hbm, again_in), load(mgain_hbm, mgain_in),
    ]
    tok_loads = []
    first = []
    rest = []
    for i in range(4):
        rows = slice(i * 256, i * 256 + 256)
        tok_loads.append(load(tok_in.at[rows], tok.at[rows]))
        if i == 0:
            for n, ref in ((0, wq_in), (1, wk_in), (2, wv_in), (3, wmk_in)):
                first.append(load(ref, w.at[:, n * 128 : n * 128 + 128]))
    for n, ref in ((4, wmq_in), (5, wmv_in), (6, wmo_in)):
        rest.append(load(ref, w.at[:, n * 128 : n * 128 + 128]))
    own_decay = load(decay_in, decays.at[k])

    barrier = pltpu.get_barrier_semaphore()
    me = r * N_TP + t

    def greet(n, _):
        other = (me + n) % (N_SP * N_TP)
        pl.semaphore_signal(
            barrier, inc=1, device_id=(other // N_TP, other % N_TP), device_id_type=MESH
        )
        return 0

    lax.fori_loop(1, N_SP * N_TP, greet, 0)

    for copy in small:
        copy.wait()
    for copy in first:
        copy.wait()

    def unit(v):
        return (v * lax.rsqrt(jnp.mean(v * v, axis=0, keepdims=True) + EPS)).astype(bf16)

    def turned(p):
        return p.astype(bf16).astype(f32).T

    for i in range(4):
        rows = slice(i * 256, i * 256 + 256)
        tok_loads[i].wait()
        v = tok[rows].astype(f32)
        ms = jnp.mean(v * v, axis=-1, keepdims=True)
        n = (v * lax.rsqrt(ms + EPS) * ngain[...]).astype(bf16)
        tok[rows] = n
        p = dot(n, w[:, 0:256])
        pq, pk = turned(p[:, :128]), turned(p[:, 128:])
        for h in range(2):
            qs[h, :, rows] = unit(pq[h * AD : h * AD + AD])
            kvs[h, 0:AD, rows] = unit(pk[h * AD : h * AD + AD])
        p = dot(n, w[:, 256:512])
        pv = turned(p[:, :128]).astype(bf16)
        for h in range(2):
            kvs[h, AD : 2 * AD, rows] = pv[h * AD : h * AD + AD]
        mk_in[rows] = p[:, 128:].astype(bf16)

    pl.semaphore_wait(barrier, N_SP * N_TP - 1)

    def worker(chunk):
        quarter, low = chunk // 4, chunk % 4
        wa_ = jnp.where(quarter % 2 == 0, low, 3 - low)
        wb = jnp.where((quarter == 0) | (quarter == 3), 0, 1)
        slot = jnp.where(quarter >= 2, 0, 1)
        return wa_, wb, slot

    my_a, my_b, my_slot = worker(r)

    def q_copy(h):
        sp, tp = chip_of(2 * k + h, my_a), 2 * x + my_b
        own = (sp == r) & (tp == t)
        return own, pltpu.make_async_remote_copy(
            qs.at[h], qb.at[my_slot], q_s.at[h], q_r.at[my_slot],
            device_id=(sp, tp), device_id_type=MESH,
        )

    def kv_copy(h):
        block = 2 * k + h
        z = jnp.where(rz // 2 == block // 2, rz, 3 - rz)
        y = jnp.where(ry // 2 == block % 2, ry, 3 - ry)
        sp, tp = 4 * z + y, 2 * x + core_for(r)
        own = (sp == r) & (tp == t)
        return own, pltpu.make_async_remote_copy(
            kvs.at[h], kv.at[r, 0 : 2 * AD], kv_s.at[h], kv_r.at[r],
            device_id=(sp, tp), device_id_type=MESH,
        )

    def decay_copy():
        return pltpu.make_async_remote_copy(
            decay_in, decays.at[k], d_s, d_r, device_id=(r, 2 * x + 1 - k), device_id_type=MESH
        )

    decay_copy().start()
    for h in range(2):
        own, copy = q_copy(h)

        @pl.when(jnp.logical_not(own))
        def _():
            copy.start()

        @pl.when(own)
        def _():
            qb[my_slot] = qs[h]

    for h in range(2):
        own, copy = kv_copy(h)

        @pl.when(jnp.logical_not(own))
        def _():
            copy.start()

        @pl.when(own)
        def _():
            kv[r, 0 : 2 * AD] = kvs[h]

    def peer(p):
        z = flip(rz) if p // 2 else rz
        y = flip(ry) if p % 2 else ry
        return 4 * z + y, member(z, y)

    def block_copy(p):
        chip, its_a = peer(p)
        wanted = (g // 2 == k) & (r <= 15 - its_a)
        return wanted, pltpu.make_async_remote_copy(
            kvs.at[g % 2], kv.at[r, 0 : 2 * AD], p_s.at[0, p - 1], kv_r.at[r],
            device_id=(chip, 2 * x + core_for(r)), device_id_type=MESH,
        )

    def block_start(p):
        wanted, copy = block_copy(p)

        @pl.when(wanted)
        def _():
            copy.start()

    block_start(1)
    block_start(2)

    w[:, 896:1024] = jnp.zeros((2048, 128), bf16)
    w[:, 896:904] = ing[...].astype(f32).T.astype(bf16)
    for copy in rest:
        copy.wait()
    gates = []
    for i in range(4):
        rows = slice(i * 256, i * 256 + 256)
        p = dot(tok[rows], w[:, 512:768])
        mq_in[:, rows] = turned(p[:, :128]).astype(bf16)
        mext[0:MD, rows] = turned(p[:, 128:]).astype(bf16)
        p = dot(tok[rows], w[:, 768:1024])
        mo_in[:, rows] = turned(p[:, :128]).astype(bf16)
        gates.append(p[:, 128:].T[0:8])

    gate8 = jnp.concatenate(gates, axis=1)
    gate = jnp.sum(
        jnp.where(lax.broadcasted_iota(jnp.int32, (8, ROWS), 0) == t, gate8, 0.0),
        axis=0, keepdims=True,
    ) + shift_ref[t]
    fade = scan_lanes(jnp.broadcast_to(fade_in[...], (8, ROWS)), jnp.add, 0.0)
    level = jnp.broadcast_to(gate, (8, ROWS)) - fade
    crest8 = scan_lanes(level, jnp.maximum, FAR)
    fade_s[...] = fade
    crest_s[...] = crest8
    levels[...] = level.T
    crest = crest8[0:1]
    top = crest[:, ROWS - 1 : ROWS]
    total = fade[0:1, ROWS - 1 : ROWS]
    mext[MD:ZR] = jnp.ones((16, ROWS), bf16)
    weighted = mext[...].astype(f32) * jnp.exp(level[0:1] - top)
    w_hi, w_lo = halves(weighted)
    z = dot(w_hi, mk_in[...]) + dot(w_lo, mk_in[...])
    def written(state, stab, faded):
        packed = (
            *pieces(state[MD : MD + 1]),
            *pieces(jnp.broadcast_to(stab, (1, MD))),
            *pieces(jnp.broadcast_to(faded, (1, MD))),
        )
        return jnp.concatenate([state[0:MD], rows_of(packed, 16, MD)], axis=0).astype(bf16)

    def read(block):
        rest = block[MD:ZR].astype(f32)
        norm = rest[0:1] + rest[1:2] + rest[2:3]
        state = jnp.concatenate(
            [block[0:MD].astype(f32), jnp.broadcast_to(norm, (16, MD))], axis=0
        )
        return state, rest[3:4] + rest[4:5] + rest[5:6], rest[6:7] + rest[7:8] + rest[8:9]

    def joined(state, log, block):
        added, stab, faded = read(block)
        log = log + faded
        new = jnp.maximum(log, stab)
        return state * jnp.exp(log - new) + added * jnp.exp(stab - new), new, faded

    zstage[...] = written(z, total + top, total)
    zb[ry] = zstage[...]

    def z_copy(to):
        return pltpu.make_async_remote_copy(
            zstage, zb.at[ry], z_s.at[to], z_r.at[ry],
            device_id=(4 * rz + to, t), device_id_type=MESH,
        )

    def row_copy(to):
        return pltpu.make_async_remote_copy(
            rowstage, rowb.at[rz], row_s.at[to], row_r.at[rz],
            device_id=(4 * to + ry, t), device_id_type=MESH,
        )

    def z_send(to, _):
        @pl.when(to != ry)
        def _():
            z_copy(to).start()

        return 0

    def row_send(to, _):
        row_copy(to).start()
        return 0

    def row_total():
        def take_in(n, _):
            @pl.when(n != ry)
            def _():
                pltpu.make_async_remote_copy(
                    zstage, zb.at[n], z_s.at[0], z_r.at[n],
                    device_id=(4 * rz, t), device_id_type=MESH,
                ).wait_recv()

            return 0

        lax.fori_loop(0, 4, take_in, 0)
        state, stab, faded = read(zb[0])
        for n in range(1, 4):
            state, stab, more = joined(state, stab, zb[n])
            faded = faded + more
        rowstage[...] = written(state, stab, faded)
        lax.fori_loop(rz + 1, 4, row_send, 0)

    def chunk_at(n):
        p = jnp.where(
            n < 4, 0, jnp.where(n < 7, n - 3, jnp.where(n < 13, (n - 5) // 2, n - 12))
        )
        m = jnp.where(n < 4, n, jnp.where(n < 7, 0, jnp.where(n < 13, 1 + (n - 7) % 2, 3)))
        pz = jnp.where(p // 2 == 1, flip(rz), rz)
        py = jnp.where(p % 2 == 1, flip(ry), ry)
        cz = jnp.where(m // 2 == 1, 3 - pz, pz)
        cy = jnp.where(m % 2 == 1, 3 - py, py)
        return 4 * cz + cy

    def sibling_uses(chunk):
        return jnp.where(b == 0, chunk <= 8 + a, chunk <= 15 - a)

    def forward_copy(chunk):
        return pltpu.make_async_remote_copy(
            kv.at[chunk, 0 : 2 * AD], kv.at[chunk, 0 : 2 * AD], f_s.at[chunk], kv_r.at[chunk],
            device_id=(r, 2 * x + 1 - k), device_id_type=MESH,
        )

    def peer_copy(chunk, n, p):
        chip, its_a = peer(p)
        return (chunk <= 15 - its_a), pltpu.make_async_remote_copy(
            kv.at[chunk, 0 : 2 * AD], kv.at[chunk, 0 : 2 * AD], p_s.at[n % 4, p - 1], kv_r.at[chunk],
            device_id=(chip, t), device_id_type=MESH,
        )

    def arrive(n, entry):
        chunk = chunk_at(n)
        mine = core_for(chunk) == b
        used = jnp.where(mine, True, jnp.where(b == 0, chunk <= 15 - a, chunk <= 8 + a))
        reaches = True if entry else chunk <= 15 - a
        own = (chunk == r) & (g // 2 == k) & mine

        @pl.when(reaches & used & jnp.logical_not(own))
        def _():
            forward_copy(chunk).wait_recv()

        @pl.when(reaches & mine)
        def _():
            @pl.when(sibling_uses(chunk))
            def _():
                forward_copy(chunk).start()

    lax.fori_loop(0, 4, z_send, 0)

    for j in range(ROWS // QT):
        cols = slice(j * QT, j * QT + QT)
        n_keys = j * QT + QT
        raw = dot(mk_in[0:n_keys], mq_in[:, cols]) * MD**-0.5
        log = levels[0:n_keys, 0:1] - crest[:, cols]
        key_at = lax.broadcasted_iota(jnp.int32, (n_keys, QT), 0)
        query_at = lax.broadcasted_iota(jnp.int32, (n_keys, QT), 1) + j * QT
        seen = key_at <= query_at
        pair = jnp.where(seen, raw * jnp.exp(jnp.where(seen, log, 0.0)), 0.0)
        p_hi, p_lo = halves(pair)
        mnum[:, cols] = dot(mext[:, 0:n_keys], p_hi) + dot(mext[:, 0:n_keys], p_lo)

    def push(n, peers):
        chunk = chunk_at(n)
        for p in peers:
            wanted, copy = peer_copy(chunk, n, p)

            @pl.when(wanted & (core_for(chunk) == b))
            def _():
                copy.start()

    arrive(0, True)
    block_start(3)
    for n in (1, 2):
        arrive(n, True)
        push(n, (1, 2))

    w_copies = []
    for n in range(8):
        rows = slice(n % 4 * 256, n % 4 * 256 + 256)
        src, dst = ((wa_in, wa), (wm_in, wm))[n // 4]
        w_copies.append(pltpu.make_async_copy(src.at[rows], dst.at[rows], wsem.at[n]))
        w_copies[-1].start()
    own_decay.wait()
    decay_copy().wait_recv()
    factor = scale_ref[head] * (AD**-0.5 * LOG2E)

    def decay_of(chunk):
        slab = decays[g // 2, :, pl.ds(pl.multiple_of(chunk * ROWS, ROWS), ROWS)]
        return jnp.where(g % 2 == 0, slab[0:1], slab[1:2]) * LOG2E

    for slot in range(2):
        chunk = hi if slot == 0 else lo
        own = (chunk == r) & (g // 2 == k)

        @pl.when(jnp.logical_not(own))
        def _():
            pltpu.make_async_remote_copy(
                qs.at[0], qb.at[slot], q_s.at[0], q_r.at[slot],
                device_id=(r, 2 * x + 1 - k), device_id_type=MESH,
            ).wait_recv()

        q_hi, q_mid, q_lo = pieces(qb[slot].astype(f32) * factor)
        d_hi, d_mid, d_lo = pieces(decay_of(chunk))
        qaug[slot, 0:64] = q_hi.astype(bf16)
        qaug[slot, 64:80] = rows_of((-1.0, -1.0, -1.0, d_hi, d_mid, d_lo), 16, ROWS).astype(bf16)
        qaug[slot, 80:128] = jnp.zeros((48, ROWS), bf16)
        qaug[slot, 128:192] = q_mid.astype(bf16)
        qaug[slot, 192:256] = q_lo.astype(bf16)
        best[slot] = jnp.full((8, ROWS), FAR, f32)
        acc[slot] = jnp.zeros((VEXT, ROWS), f32)

    def ones_row(chunk, _):
        kv[chunk, 2 * AD : 2 * AD + 16] = jnp.ones((16, ROWS), bf16)
        return 0

    lax.fori_loop(0, N_SP, ones_row, 0)

    def fold(slot, chunk, diag):
        def scores(i):
            cols = slice(i * QT, i * QT + QT)
            out = []
            for j in range(i + 1 if diag else ROWS // QT):
                s = dot(kaug[j * QT : j * QT + QT], qaug[slot, :, cols])
                if diag and j == i:
                    key_at = lax.broadcasted_iota(jnp.int32, (QT, QT), 0)
                    query_at = lax.broadcasted_iota(jnp.int32, (QT, QT), 1)
                    s = jnp.where(key_at <= query_at, s, FAR)
                out.append(s)
            return out

        def finish(i, parts):
            cols = slice(i * QT, i * QT + QT)
            old = best[slot, 0:1, cols]
            tops = parts[0]
            for s in parts[1:]:
                tops = jnp.maximum(tops, s)
            new = jnp.maximum(old, jnp.max(tops, axis=0, keepdims=True))
            got = jnp.zeros((VEXT, QT), f32)
            for j, s in enumerate(parts):
                weights = jnp.exp2(s - new).astype(bf16)
                got = got + dot(kv[chunk, AD : AD + VEXT, j * QT : j * QT + QT], weights)
            acc[slot, :, cols] = acc[slot, :, cols] * jnp.exp2(old - new) + got
            best[slot, 0:1, cols] = new

        tiles = ROWS // QT
        s = scores(0)
        for i in range(tiles):
            later = scores(i + 1) if i + 1 < tiles else None
            finish(i, s)
            s = later

    def m_copy(p):
        return pltpu.make_async_remote_copy(
            mstage.at[p], mb.at[t], m_s.at[p], m_r.at[t], device_id=(r, p), device_id_type=MESH
        )

    def m_send(p, _):
        @pl.when(p != t)
        def _():
            m_copy(p).start()

        @pl.when(p == t)
        def _():
            mb[t] = mstage[p]

        return 0

    def recall():
        z0 = jnp.concatenate(
            [cinit_in[0].T, jnp.broadcast_to(ninit_in[...], (16, MD))], axis=0
        )

        def enter_row(n, carry):
            pltpu.make_async_remote_copy(
                rowstage, rowb.at[n], row_s.at[0], row_r.at[n],
                device_id=(ry, t), device_id_type=MESH,
            ).wait_recv()
            return joined(*carry, rowb[n])[:2]

        def enter(n, carry):
            return joined(*carry, zb[n])[:2]

        carry = lax.fori_loop(0, rz, enter_row, (z0, jnp.zeros((1, MD), f32)))
        state, log = lax.fori_loop(0, ry, enter, carry)
        crest = crest_s[0:1]
        log = log[:, 0:1]
        peak = jnp.maximum(crest, log)
        s_hi, s_lo = halves(state)
        carried = (dot(s_hi, mq_in[...]) + dot(s_lo, mq_in[...])) * MD**-0.5
        numer = mnum[...] * jnp.exp(crest - peak) + carried * jnp.exp(log - peak)
        floor = jnp.exp(-(fade_s[0:1] + peak))
        recalled = numer[0:MD] / jnp.maximum(jnp.abs(numer[MD : MD + 1]), floor)
        squares = jnp.sum(recalled * recalled, axis=0, keepdims=True)
        sq_hi, sq_mid, sq_lo = pieces(squares)
        gated = (recalled * jax.nn.sigmoid(mo_in[...].astype(f32))).astype(bf16)
        stats = rows_of((sq_hi, sq_mid, sq_lo), 16, ROWS).astype(bf16)
        for p in range(N_TP):
            mstage[p, 0:MD] = gated[:, p * 128 : p * 128 + 128]
            mstage[p, MD:ZR] = stats[:, p * 128 : p * 128 + 128]

        lax.fori_loop(0, N_TP, m_send, 0)

    def o_copy(slot, p):
        chunk = hi if slot == 0 else lo
        own = (chunk == r) & (p == t)
        return own, pltpu.make_async_remote_copy(
            ostage.at[slot, p], att.at[head], o_s.at[slot, p], o_r.at[head],
            device_id=(chunk, p), device_id_type=MESH,
        )

    def depart(slot):
        result = acc[slot, 0:AD] / acc[slot, AD : AD + 1]
        result = result.astype(bf16)
        for p in range(N_TP):
            ostage[slot, p] = result[:, p * 128 : p * 128 + 128]

        def o_send(p, _):
            own, copy = o_copy(slot, p)

            @pl.when(jnp.logical_not(own))
            def _():
                copy.start()

            @pl.when(own)
            def _():
                att[head] = ostage[slot, p]

            return 0

        lax.fori_loop(0, N_TP, o_send, 0)

    def next_one(j, _):
        arrive(j, False)
        return 0

    def visit(n, carry):
        early, ahead = carry
        lax.fori_loop(ahead, n + 1, next_one, 0)
        ahead = jnp.maximum(ahead, n + 1)
        chunk = chunk_at(n)

        @pl.when(chunk <= hi)
        def _():
            take(chunk, n, ahead)

        early = early + jnp.where(chunk <= lo, 1, 0)

        @pl.when((chunk <= lo) & (early == lo + 1))
        def _():
            depart(1)

        @pl.when(n == 0)
        def _():
            push(1, (3,))
            push(2, (3,))
            arrive(3, True)

        @pl.when(n == 1)
        def _():
            push(3, (1, 2))

        @pl.when(n == 2)
        def _():
            push(3, (3,))

        @pl.when(n == ROW_AT)
        def _():
            row_total()

        @pl.when(n == RECALL_AT)
        def _():
            recall()

        folds = jnp.where(chunk <= hi, 1, 0) + jnp.where(chunk <= lo, 1, 0)
        return early, jnp.minimum(ahead + jnp.where(n >= 2, folds, 0), N_SP)

    def take(chunk, n, ahead):
        keys = kv[chunk, 0:AD]
        d_hi, d_mid, d_lo = pieces(decay_of(chunk))
        extra = rows_of((d_hi, d_mid, d_lo, 1.0, 1.0, 1.0), 64, ROWS)
        kaug[:, 0:128] = jnp.concatenate([keys, extra.astype(bf16)], axis=0).T
        kaug[:, 128:256] = jnp.concatenate([keys, keys], axis=0).T

        def side(slot, _):
            mine = jnp.where(slot == 0, hi, lo)

            @pl.when(chunk < mine)
            def _():
                fold(slot, chunk, False)

            @pl.when(chunk == mine)
            def _():
                fold(slot, chunk, True)

            @pl.when((chunk <= mine) & (n >= 2) & (ahead + slot < N_SP))
            def _():
                arrive(ahead + slot, False)

            return 0

        lax.fori_loop(0, 2, side, 0)

    lax.fori_loop(0, 16, visit, (0, 4))

    depart(0)

    def o_wait(n, _):
        own = (n == head) & ((hi == r) | (lo == r))

        @pl.when(jnp.logical_not(own))
        def _():
            pltpu.make_async_remote_copy(
                ostage.at[0, 0], att.at[n], o_s.at[0, 0], o_r.at[n],
                device_id=(r, (t + 1) % N_TP), device_id_type=MESH,
            ).wait_recv()

        return 0

    def m_wait(n, _):
        @pl.when(n != t)
        def _():
            pltpu.make_async_remote_copy(
                mstage.at[0], mb.at[n], m_s.at[0], m_r.at[n],
                device_id=(r, (t + 1) % N_TP), device_id_type=MESH,
            ).wait_recv()

        return 0

    lax.fori_loop(0, N_TP, m_wait, 0)
    for copy in w_copies:
        copy.wait()

    m_all = jnp.concatenate([mb[n, 0:MD].astype(f32).T for n in range(N_TP)], axis=1)
    m_stats = sum(mb[n, MD:ZR].astype(f32) for n in range(N_TP)).T
    m_sq = m_stats[:, 0:1] + m_stats[:, 1:2] + m_stats[:, 2:3]
    m_mix = (m_all * lax.rsqrt(m_sq / 1024.0 + EPS) * mgain_in[...]).astype(bf16)

    for n in range(4):
        cols = slice(n * 512, n * 512 + 512)
        half[:, cols] = dot(m_mix, wm[:, cols])

    decay_copy().wait_send()
    for h in range(2):
        for own, copy in (q_copy(h), kv_copy(h)):

            @pl.when(jnp.logical_not(own))
            def _():
                copy.wait_send()

    for p in (1, 2, 3):
        wanted, copy = block_copy(p)

        @pl.when(wanted)
        def _():
            copy.wait_send()

    def z_done(to, _):
        @pl.when(to != ry)
        def _():
            z_copy(to).wait_send()

        return 0

    def row_done(to, _):
        row_copy(to).wait_send()
        return 0

    lax.fori_loop(0, 4, z_done, 0)
    lax.fori_loop(rz + 1, 4, row_done, 0)

    def f_done(n, _):
        chunk = chunk_at(n)
        mine = core_for(chunk) == b
        reaches = jnp.where(n < 4, True, chunk <= 15 - a)

        @pl.when(reaches & mine)
        def _():
            @pl.when((n > 0) & (n < 4))
            def _():
                for p in (1, 2, 3):
                    wanted, copy = peer_copy(chunk, n, p)

                    @pl.when(wanted)
                    def _():
                        copy.wait_send()

            @pl.when(sibling_uses(chunk))
            def _():
                forward_copy(chunk).wait_send()

        return 0

    lax.fori_loop(0, N_SP, f_done, 0)

    lax.fori_loop(0, 16, o_wait, 0)
    a_all = jnp.concatenate(
        [
            jnp.concatenate([att[2 * n], att[2 * n + 1]], axis=0).astype(f32).T
            for n in range(8)
        ],
        axis=1,
    )
    a_sq = jnp.sum(a_all * a_all, axis=1, keepdims=True)
    a_mix = (a_all * lax.rsqrt(a_sq / 1024.0 + EPS) * again_in[...]).astype(bf16)
    for n in range(4):
        cols = slice(n * 512, n * 512 + 512)
        out[:, cols] = (half[:, cols] + dot(a_mix, wa[:, cols])).astype(bf16)

    def p_done(p, _):
        for slot in range(2):
            own, copy = o_copy(slot, p)

            @pl.when(jnp.logical_not(own))
            def _():
                copy.wait_send()

        @pl.when(p != t)
        def _():
            m_copy(p).wait_send()

        return 0

    lax.fori_loop(0, N_TP, p_done, 0)


def mix(*arrays):
    smem = pl.BlockSpec(memory_space=pltpu.SMEM)
    hbm = pl.BlockSpec(memory_space=pltpu.HBM)
    dma = pltpu.SemaphoreType.DMA
    return pl.pallas_call(
        mix_kernel,
        out_shape=jax.ShapeDtypeStruct((128, 2048), bf16),
        in_specs=[smem] * 2 + [hbm] * 18,
        out_specs=pl.BlockSpec(memory_space=pltpu.VMEM),
        scratch_shapes=[
            pltpu.VMEM((ROWS, 2048), bf16),
            pltpu.VMEM((2048, 1024), bf16),
            pltpu.VMEM((8, 2048), bf16),
            pltpu.VMEM((1, 2048), f32),
            pltpu.VMEM((1, ROWS), f32),
            pltpu.VMEM((1, MD, MD), f32),
            pltpu.VMEM((1, MD), f32),
            pltpu.VMEM((1, 1024), f32),
            pltpu.VMEM((1, 1024), f32),
            pltpu.VMEM((2, AD, ROWS), bf16),
            pltpu.VMEM((2, 2 * AD, ROWS), bf16),
            pltpu.VMEM((MD, ROWS), bf16),
            pltpu.VMEM((ROWS, MD), bf16),
            pltpu.VMEM((MD, ROWS), bf16),
            pltpu.VMEM((8, ROWS), f32),
            pltpu.VMEM((8, ROWS), f32),
            pltpu.VMEM((ROWS, 8), f32),
            pltpu.VMEM((1024, 2048), bf16),
            pltpu.VMEM((1024, 2048), bf16),
            pltpu.VMEM((N_SP, 2 * AD + 16, ROWS), bf16),
            pltpu.VMEM((2, AD, ROWS), bf16),
            pltpu.VMEM((2, 2, N_SP * ROWS), f32),
            pltpu.VMEM((ROWS, 256), bf16),
            pltpu.VMEM((2, 256, ROWS), bf16),
            pltpu.VMEM((2, 8, ROWS), f32),
            pltpu.VMEM((2, VEXT, ROWS), f32),
            pltpu.VMEM((2, N_TP, AD, 128), bf16),
            pltpu.VMEM((16, AD, 128), bf16),
            pltpu.VMEM((ZR, MD), bf16),
            pltpu.VMEM((4, ZR, MD), bf16),
            pltpu.VMEM((ZR, MD), bf16),
            pltpu.VMEM((4, ZR, MD), bf16),
            pltpu.VMEM((N_TP, ZR, 128), bf16),
            pltpu.VMEM((N_TP, ZR, 128), bf16),
            pltpu.VMEM((ZR, ROWS), bf16),
            pltpu.VMEM((ZR, ROWS), f32),
            pltpu.VMEM((128, 2048), f32),
            dma((20,)), dma((8,)),
            dma((2,)), dma((N_SP,)),
            dma((2,)), dma((2,)),
            dma((4,)), dma((4,)), dma((4,)), dma((4,)),
            dma((N_TP,)), dma((N_TP,)),
            dma((2, N_TP)), dma((16,)),
            dma((4, 3)), dma((N_SP,)), dma, dma,
        ],
        compiler_params=pltpu.CompilerParams(
            collective_id=0, has_side_effects=True, vmem_limit_bytes=60 * 2**20
        ),
        cost_estimate=pl.CostEstimate(
            flops=60 * 10**9, bytes_accessed=12 * 2**20, transcendentals=0
        ),
    )(*arrays)


def on_device(tokens, norm_gain, attn_query, attn_key, attn_value, score_scale, attention_decay,
              mem_query, mem_key, mem_value, mem_ingate, input_shift, memory_decay, mem_outgate,
              init_memory, init_normalizer, attn_gain, mem_gain, attn_out, mem_out):
    return mix(
        score_scale, input_shift, tokens, attn_query, attn_key, attn_value, mem_query, mem_key,
        mem_value, mem_outgate, mem_ingate.T, norm_gain.reshape(1, 2048), memory_decay,
        attention_decay, init_memory, init_normalizer, attn_gain.reshape(1, 1024),
        mem_gain.reshape(1, 1024), attn_out, mem_out,
    )


def solution(mesh):
    tp = P(None, "tp")
    placed = (
        P("sp", None), P(), tp, tp, tp, P(), P("tp", None), tp, tp, tp, P(), P(),
        P("tp", "sp"), tp, P("tp", None, None), P("tp", None), P(), P(), P(), P(),
    )
    return jax.shard_map(
        on_device, mesh=mesh, in_specs=placed, out_specs=P(("sp", "tp"), None), check_vma=False
    )
```

```python
import functools
import math

import jax
import jax.numpy as jnp
from jax import lax
from jax.experimental import pallas as pl
from jax.experimental.pallas import tpu as pltpu
from jax.sharding import PartitionSpec as P

MESH = pl.DeviceIdType.MESH
f32 = jnp.float32
bf16 = jnp.bfloat16
EPS = 1e-06
LOG2E = math.log2(math.e)
FAR = -1e30
ROWS = 1024
AD = 64
MD = 128
QT = 256
N_SP, N_TP = 16, 8
ROW_AT = 7
RECALL_AT = 12
VEXT = AD + 16
ZR = MD + 16


def dot(a, b):
    return jnp.dot(a, b, preferred_element_type=f32)


def pieces(x):
    hi = x.astype(bf16).astype(f32)
    rest = x - hi
    mid = rest.astype(bf16).astype(f32)
    low = (rest - mid).astype(bf16).astype(f32)
    return hi, mid, low


def halves(x):
    hi = x.astype(bf16)
    return hi, (x - hi.astype(f32)).astype(bf16)


def rows_of(values, height, width):
    at = lax.broadcasted_iota(jnp.int32, (height, width), 0)
    out = jnp.zeros((height, width), f32)
    for n, value in enumerate(values):
        out = jnp.where(at == n, value, out)
    return out


def shifted(x, by, fill):
    at = lax.broadcasted_iota(jnp.int32, x.shape, 1)
    return jnp.where(at >= by, pltpu.roll(x, by, 1), fill)


def scan_lanes(x, join, fill):
    by = 1
    while by < x.shape[1]:
        x = join(x, shifted(x, by, fill))
        by *= 2
    return x


def mix_kernel(scale_ref, shift_ref, tok_in, wq_in, wk_in, wv_in, wmq_in, wmk_in, wmv_in, wmo_in, ing_in,
               ngain_in, fade_hbm, decay_in, cinit_hbm, ninit_hbm, again_hbm, mgain_hbm, wa_in, wm_in,
               out, tok, w, ing, ngain, fade_in, cinit_in, ninit_in, again_in, mgain_in,
               qs, kvs, mq_in, mk_in, mo_in, fade_s, crest_s, levels,
               wa, wm, kv, qb, decays, kaug, qaug, best, acc, ostage, att,
               zstage, zb, rowstage, rowb, mstage, mb, mext, mnum, half,
               isem, wsem, kv_s, kv_r, q_s, q_r, z_s, z_r, row_s, row_r, m_s, m_r, o_s, o_r, p_s, f_s, d_s, d_r):
    r = lax.axis_index("sp")
    t = lax.axis_index("tp")
    x, k = t // 2, t % 2
    rz, ry = r // 4, r % 4

    def member(z, y):
        m = 2 * (z % 2) + y % 2
        return jnp.where(z // 2 == 1, 3 - m, m)

    g = 2 * (rz // 2) + ry // 2
    a = member(rz, ry)
    b = k
    hi = jnp.where(b == 0, 15 - a, 8 + a)
    lo = jnp.where(b == 0, a, 7 - a)
    head = 4 * x + g

    def chip_of(block, member):
        m = jnp.where(block // 2 == 1, 3 - member, member)
        return 4 * (2 * (block // 2) + m // 2) + 2 * (block % 2) + m % 2

    def flip(v):
        return v + 1 - 2 * (v % 2)

    def core_for(chunk):
        return (chunk % 4) // 2

    loads = []

    def load(src, dst):
        copy = pltpu.make_async_copy(src, dst, isem.at[len(loads)])
        copy.start()
        loads.append(copy)
        return copy

    small = [
        load(ngain_in, ngain), load(ing_in, ing), load(fade_hbm, fade_in), load(cinit_hbm, cinit_in),
        load(ninit_hbm, ninit_in), load(again_hbm, again_in), load(mgain_hbm, mgain_in),
    ]
    tok_loads = []
    first = []
    rest = []
    for i in range(4):
        rows = slice(i * 256, i * 256 + 256)
        tok_loads.append(load(tok_in.at[rows], tok.at[rows]))
        if i == 0:
            for n, ref in ((0, wq_in), (1, wk_in), (2, wv_in), (3, wmk_in)):
                first.append(load(ref, w.at[:, n * 128 : n * 128 + 128]))
    for n, ref in ((4, wmq_in), (5, wmv_in), (6, wmo_in)):
        rest.append(load(ref, w.at[:, n * 128 : n * 128 + 128]))
    own_decay = load(decay_in, decays.at[k])

    barrier = pltpu.get_barrier_semaphore()
    me = r * N_TP + t

    def greet(n, _):
        other = (me + n) % (N_SP * N_TP)
        pl.semaphore_signal(
            barrier, inc=1, device_id=(other // N_TP, other % N_TP), device_id_type=MESH
        )
        return 0

    lax.fori_loop(1, N_SP * N_TP, greet, 0)

    for copy in small:
        copy.wait()
    for copy in first:
        copy.wait()

    def unit(v):
        return (v * lax.rsqrt(jnp.mean(v * v, axis=0, keepdims=True) + EPS)).astype(bf16)

    def turned(p):
        return p.astype(bf16).astype(f32).T

    for i in range(4):
        rows = slice(i * 256, i * 256 + 256)
        tok_loads[i].wait()
        v = tok[rows].astype(f32)
        ms = jnp.mean(v * v, axis=-1, keepdims=True)
        n = (v * lax.rsqrt(ms + EPS) * ngain[...]).astype(bf16)
        tok[rows] = n
        p = dot(n, w[:, 0:256])
        pq, pk = turned(p[:, :128]), turned(p[:, 128:])
        for h in range(2):
            qs[h, :, rows] = unit(pq[h * AD : h * AD + AD])
            kvs[h, 0:AD, rows] = unit(pk[h * AD : h * AD + AD])
        p = dot(n, w[:, 256:512])
        pv = turned(p[:, :128]).astype(bf16)
        for h in range(2):
            kvs[h, AD : 2 * AD, rows] = pv[h * AD : h * AD + AD]
        mk_in[rows] = p[:, 128:].astype(bf16)

    pl.semaphore_wait(barrier, N_SP * N_TP - 1)

    def worker(chunk):
        quarter, low = chunk // 4, chunk % 4
        wa_ = jnp.where(quarter % 2 == 0, low, 3 - low)
        wb = jnp.where((quarter == 0) | (quarter == 3), 0, 1)
        slot = jnp.where(quarter >= 2, 0, 1)
        return wa_, wb, slot

    my_a, my_b, my_slot = worker(r)

    def q_copy(h):
        sp, tp = chip_of(2 * k + h, my_a), 2 * x + my_b
        own = (sp == r) & (tp == t)
        return own, pltpu.make_async_remote_copy(
            qs.at[h], qb.at[my_slot], q_s.at[h], q_r.at[my_slot],
            device_id=(sp, tp), device_id_type=MESH,
        )

    def kv_copy(h):
        block = 2 * k + h
        z = jnp.where(rz // 2 == block // 2, rz, 3 - rz)
        y = jnp.where(ry // 2 == block % 2, ry, 3 - ry)
        sp, tp = 4 * z + y, 2 * x + core_for(r)
        own = (sp == r) & (tp == t)
        return own, pltpu.make_async_remote_copy(
            kvs.at[h], kv.at[r, 0 : 2 * AD], kv_s.at[h], kv_r.at[r],
            device_id=(sp, tp), device_id_type=MESH,
        )

    def decay_copy():
        return pltpu.make_async_remote_copy(
            decay_in, decays.at[k], d_s, d_r, device_id=(r, 2 * x + 1 - k), device_id_type=MESH
        )

    decay_copy().start()
    for h in range(2):
        own, copy = q_copy(h)

        @pl.when(jnp.logical_not(own))
        def _():
            copy.start()

        @pl.when(own)
        def _():
            qb[my_slot] = qs[h]

    for h in range(2):
        own, copy = kv_copy(h)

        @pl.when(jnp.logical_not(own))
        def _():
            copy.start()

        @pl.when(own)
        def _():
            kv[r, 0 : 2 * AD] = kvs[h]

    def peer(p):
        z = flip(rz) if p // 2 else rz
        y = flip(ry) if p % 2 else ry
        return 4 * z + y, member(z, y)

    def block_copy(p):
        chip, its_a = peer(p)
        wanted = (g // 2 == k) & (r <= 15 - its_a)
        return wanted, pltpu.make_async_remote_copy(
            kvs.at[g % 2], kv.at[r, 0 : 2 * AD], p_s.at[0, p - 1], kv_r.at[r],
            device_id=(chip, 2 * x + core_for(r)), device_id_type=MESH,
        )

    def block_start(p):
        wanted, copy = block_copy(p)

        @pl.when(wanted)
        def _():
            copy.start()

    block_start(1)
    block_start(2)

    w[:, 896:1024] = jnp.zeros((2048, 128), bf16)
    w[:, 896:904] = ing[...].astype(f32).T.astype(bf16)
    for copy in rest:
        copy.wait()
    gates = []
    for i in range(4):
        rows = slice(i * 256, i * 256 + 256)
        p = dot(tok[rows], w[:, 512:768])
        mq_in[:, rows] = turned(p[:, :128]).astype(bf16)
        mext[0:MD, rows] = turned(p[:, 128:]).astype(bf16)
        p = dot(tok[rows], w[:, 768:1024])
        mo_in[:, rows] = turned(p[:, :128]).astype(bf16)
        gates.append(p[:, 128:].T[0:8])

    gate8 = jnp.concatenate(gates, axis=1)
    gate = jnp.sum(
        jnp.where(lax.broadcasted_iota(jnp.int32, (8, ROWS), 0) == t, gate8, 0.0),
        axis=0, keepdims=True,
    ) + shift_ref[t]
    fade = scan_lanes(jnp.broadcast_to(fade_in[...], (8, ROWS)), jnp.add, 0.0)
    level = jnp.broadcast_to(gate, (8, ROWS)) - fade
    crest8 = scan_lanes(level, jnp.maximum, FAR)
    fade_s[...] = fade
    crest_s[...] = crest8
    levels[...] = level.T
    crest = crest8[0:1]
    top = crest[:, ROWS - 1 : ROWS]
    total = fade[0:1, ROWS - 1 : ROWS]
    mext[MD:ZR] = jnp.ones((16, ROWS), bf16)
    weighted = mext[...].astype(f32) * jnp.exp(level[0:1] - top)
    w_hi, w_lo = halves(weighted)
    z = dot(w_hi, mk_in[...]) + dot(w_lo, mk_in[...])
    def written(state, stab, faded):
        packed = (
            *pieces(state[MD : MD + 1]),
            *pieces(jnp.broadcast_to(stab, (1, MD))),
            *pieces(jnp.broadcast_to(faded, (1, MD))),
        )
        return jnp.concatenate([state[0:MD], rows_of(packed, 16, MD)], axis=0).astype(bf16)

    def read(block):
        rest = block[MD:ZR].astype(f32)
        norm = rest[0:1] + rest[1:2] + rest[2:3]
        state = jnp.concatenate(
            [block[0:MD].astype(f32), jnp.broadcast_to(norm, (16, MD))], axis=0
        )
        return state, rest[3:4] + rest[4:5] + rest[5:6], rest[6:7] + rest[7:8] + rest[8:9]

    def joined(state, log, block):
        added, stab, faded = read(block)
        log = log + faded
        new = jnp.maximum(log, stab)
        return state * jnp.exp(log - new) + added * jnp.exp(stab - new), new, faded

    zstage[...] = written(z, total + top, total)
    zb[ry] = zstage[...]

    def z_copy(to):
        return pltpu.make_async_remote_copy(
            zstage, zb.at[ry], z_s.at[to], z_r.at[ry],
            device_id=(4 * rz + to, t), device_id_type=MESH,
        )

    def row_copy(to):
        return pltpu.make_async_remote_copy(
            rowstage, rowb.at[rz], row_s.at[to], row_r.at[rz],
            device_id=(4 * to + ry, t), device_id_type=MESH,
        )

    def z_send(to, _):
        @pl.when(to != ry)
        def _():
            z_copy(to).start()

        return 0

    def row_send(to, _):
        row_copy(to).start()
        return 0

    def row_total():
        def take_in(n, _):
            @pl.when(n != ry)
            def _():
                pltpu.make_async_remote_copy(
                    zstage, zb.at[n], z_s.at[0], z_r.at[n],
                    device_id=(4 * rz, t), device_id_type=MESH,
                ).wait_recv()

            return 0

        lax.fori_loop(0, 4, take_in, 0)
        state, stab, faded = read(zb[0])
        for n in range(1, 4):
            state, stab, more = joined(state, stab, zb[n])
            faded = faded + more
        rowstage[...] = written(state, stab, faded)
        lax.fori_loop(rz + 1, 4, row_send, 0)

    def chunk_at(n):
        p = jnp.where(
            n < 4, 0, jnp.where(n < 7, n - 3, jnp.where(n < 13, (n - 5) // 2, n - 12))
        )
        m = jnp.where(n < 4, n, jnp.where(n < 7, 0, jnp.where(n < 13, 1 + (n - 7) % 2, 3)))
        pz = jnp.where(p // 2 == 1, flip(rz), rz)
        py = jnp.where(p % 2 == 1, flip(ry), ry)
        cz = jnp.where(m // 2 == 1, 3 - pz, pz)
        cy = jnp.where(m % 2 == 1, 3 - py, py)
        return 4 * cz + cy

    def sibling_uses(chunk):
        return jnp.where(b == 0, chunk <= 8 + a, chunk <= 15 - a)

    def forward_copy(chunk):
        return pltpu.make_async_remote_copy(
            kv.at[chunk, 0 : 2 * AD], kv.at[chunk, 0 : 2 * AD], f_s.at[chunk], kv_r.at[chunk],
            device_id=(r, 2 * x + 1 - k), device_id_type=MESH,
        )

    def peer_copy(chunk, n, p):
        chip, its_a = peer(p)
        return (chunk <= 15 - its_a), pltpu.make_async_remote_copy(
            kv.at[chunk, 0 : 2 * AD], kv.at[chunk, 0 : 2 * AD], p_s.at[n % 4, p - 1], kv_r.at[chunk],
            device_id=(chip, t), device_id_type=MESH,
        )

    def arrive(n, entry):
        chunk = chunk_at(n)
        mine = core_for(chunk) == b
        used = jnp.where(mine, True, jnp.where(b == 0, chunk <= 15 - a, chunk <= 8 + a))
        reaches = True if entry else chunk <= 15 - a
        own = (chunk == r) & (g // 2 == k) & mine

        @pl.when(reaches & used & jnp.logical_not(own))
        def _():
            forward_copy(chunk).wait_recv()

        @pl.when(reaches & mine)
        def _():
            @pl.when(sibling_uses(chunk))
            def _():
                forward_copy(chunk).start()

    lax.fori_loop(0, 4, z_send, 0)

    for j in range(ROWS // QT):
        cols = slice(j * QT, j * QT + QT)
        n_keys = j * QT + QT
        raw = dot(mk_in[0:n_keys], mq_in[:, cols]) * MD**-0.5
        log = levels[0:n_keys, 0:1] - crest[:, cols]
        key_at = lax.broadcasted_iota(jnp.int32, (n_keys, QT), 0)
        query_at = lax.broadcasted_iota(jnp.int32, (n_keys, QT), 1) + j * QT
        seen = key_at <= query_at
        pair = jnp.where(seen, raw * jnp.exp(jnp.where(seen, log, 0.0)), 0.0)
        p_hi, p_lo = halves(pair)
        mnum[:, cols] = dot(mext[:, 0:n_keys], p_hi) + dot(mext[:, 0:n_keys], p_lo)

    def push(n, peers):
        chunk = chunk_at(n)
        for p in peers:
            wanted, copy = peer_copy(chunk, n, p)

            @pl.when(wanted & (core_for(chunk) == b))
            def _():
                copy.start()

    arrive(0, True)
    block_start(3)

    w_copies = []
    for n in range(8):
        rows = slice(n % 4 * 256, n % 4 * 256 + 256)
        src, dst = ((wa_in, wa), (wm_in, wm))[n // 4]
        w_copies.append(pltpu.make_async_copy(src.at[rows], dst.at[rows], wsem.at[n]))
        w_copies[-1].start()
    own_decay.wait()
    decay_copy().wait_recv()
    factor = scale_ref[head] * (AD**-0.5 * LOG2E)

    def decay_of(chunk):
        slab = decays[g // 2, :, pl.ds(pl.multiple_of(chunk * ROWS, ROWS), ROWS)]
        return jnp.where(g % 2 == 0, slab[0:1], slab[1:2]) * LOG2E

    for slot in range(2):
        chunk = hi if slot == 0 else lo
        own = (chunk == r) & (g // 2 == k)

        @pl.when(jnp.logical_not(own))
        def _():
            pltpu.make_async_remote_copy(
                qs.at[0], qb.at[slot], q_s.at[0], q_r.at[slot],
                device_id=(r, 2 * x + 1 - k), device_id_type=MESH,
            ).wait_recv()

        q_hi, q_mid, q_lo = pieces(qb[slot].astype(f32) * factor)
        d_hi, d_mid, d_lo = pieces(decay_of(chunk))
        qaug[slot, 0:64] = q_hi.astype(bf16)
        qaug[slot, 64:80] = rows_of((-1.0, -1.0, -1.0, d_hi, d_mid, d_lo), 16, ROWS).astype(bf16)
        qaug[slot, 80:128] = jnp.zeros((48, ROWS), bf16)
        qaug[slot, 128:192] = q_mid.astype(bf16)
        qaug[slot, 192:256] = q_lo.astype(bf16)
        best[slot] = jnp.full((8, ROWS), FAR, f32)
        acc[slot] = jnp.zeros((VEXT, ROWS), f32)

    def ones_row(chunk, _):
        kv[chunk, 2 * AD : 2 * AD + 16] = jnp.ones((16, ROWS), bf16)
        return 0

    lax.fori_loop(0, N_SP, ones_row, 0)

    def fold(slot, chunk, diag):
        def scores(i):
            cols = slice(i * QT, i * QT + QT)
            out = []
            for j in range(i + 1 if diag else ROWS // QT):
                s = dot(kaug[j * QT : j * QT + QT], qaug[slot, :, cols])
                if diag and j == i:
                    key_at = lax.broadcasted_iota(jnp.int32, (QT, QT), 0)
                    query_at = lax.broadcasted_iota(jnp.int32, (QT, QT), 1)
                    s = jnp.where(key_at <= query_at, s, FAR)
                out.append(s)
            return out

        def finish(i, parts):
            cols = slice(i * QT, i * QT + QT)
            old = best[slot, 0:1, cols]
            tops = parts[0]
            for s in parts[1:]:
                tops = jnp.maximum(tops, s)
            new = jnp.maximum(old, jnp.max(tops, axis=0, keepdims=True))
            got = jnp.zeros((VEXT, QT), f32)
            for j, s in enumerate(parts):
                weights = jnp.exp2(s - new).astype(bf16)
                got = got + dot(kv[chunk, AD : AD + VEXT, j * QT : j * QT + QT], weights)
            acc[slot, :, cols] = acc[slot, :, cols] * jnp.exp2(old - new) + got
            best[slot, 0:1, cols] = new

        tiles = ROWS // QT
        s = scores(0)
        for i in range(tiles):
            later = scores(i + 1) if i + 1 < tiles else None
            finish(i, s)
            s = later

    def m_copy(p):
        return pltpu.make_async_remote_copy(
            mstage.at[p], mb.at[t], m_s.at[p], m_r.at[t], device_id=(r, p), device_id_type=MESH
        )

    def m_send(p, _):
        @pl.when(p != t)
        def _():
            m_copy(p).start()

        @pl.when(p == t)
        def _():
            mb[t] = mstage[p]

        return 0

    def recall():
        z0 = jnp.concatenate(
            [cinit_in[0].T, jnp.broadcast_to(ninit_in[...], (16, MD))], axis=0
        )

        def enter_row(n, carry):
            pltpu.make_async_remote_copy(
                rowstage, rowb.at[n], row_s.at[0], row_r.at[n],
                device_id=(ry, t), device_id_type=MESH,
            ).wait_recv()
            return joined(*carry, rowb[n])[:2]

        def enter(n, carry):
            return joined(*carry, zb[n])[:2]

        carry = lax.fori_loop(0, rz, enter_row, (z0, jnp.zeros((1, MD), f32)))
        state, log = lax.fori_loop(0, ry, enter, carry)
        crest = crest_s[0:1]
        log = log[:, 0:1]
        peak = jnp.maximum(crest, log)
        s_hi, s_lo = halves(state)
        carried = (dot(s_hi, mq_in[...]) + dot(s_lo, mq_in[...])) * MD**-0.5
        numer = mnum[...] * jnp.exp(crest - peak) + carried * jnp.exp(log - peak)
        floor = jnp.exp(-(fade_s[0:1] + peak))
        recalled = numer[0:MD] / jnp.maximum(jnp.abs(numer[MD : MD + 1]), floor)
        squares = jnp.sum(recalled * recalled, axis=0, keepdims=True)
        sq_hi, sq_mid, sq_lo = pieces(squares)
        gated = (recalled * jax.nn.sigmoid(mo_in[...].astype(f32))).astype(bf16)
        stats = rows_of((sq_hi, sq_mid, sq_lo), 16, ROWS).astype(bf16)
        for p in range(N_TP):
            mstage[p, 0:MD] = gated[:, p * 128 : p * 128 + 128]
            mstage[p, MD:ZR] = stats[:, p * 128 : p * 128 + 128]

        lax.fori_loop(0, N_TP, m_send, 0)

    def o_copy(slot, p):
        chunk = hi if slot == 0 else lo
        own = (chunk == r) & (p == t)
        return own, pltpu.make_async_remote_copy(
            ostage.at[slot, p], att.at[head], o_s.at[slot, p], o_r.at[head],
            device_id=(chunk, p), device_id_type=MESH,
        )

    def depart(slot):
        result = acc[slot, 0:AD] / acc[slot, AD : AD + 1]
        result = result.astype(bf16)
        for p in range(N_TP):
            ostage[slot, p] = result[:, p * 128 : p * 128 + 128]

        def o_send(p, _):
            own, copy = o_copy(slot, p)

            @pl.when(jnp.logical_not(own))
            def _():
                copy.start()

            @pl.when(own)
            def _():
                att[head] = ostage[slot, p]

            return 0

        lax.fori_loop(0, N_TP, o_send, 0)

    def next_one(j, _):
        arrive(j, False)
        return 0

    def visit(n, carry):
        early, ahead = carry
        lax.fori_loop(ahead, n + 1, next_one, 0)
        ahead = jnp.maximum(ahead, n + 1)
        chunk = chunk_at(n)

        @pl.when(chunk <= hi)
        def _():
            take(chunk, n, ahead)

        early = early + jnp.where(chunk <= lo, 1, 0)

        @pl.when((chunk <= lo) & (early == lo + 1))
        def _():
            depart(1)

        @pl.when(n == 0)
        def _():
            for entry in (1, 2):
                arrive(entry, True)
                push(entry, (1, 2))

        @pl.when(n == 1)
        def _():
            push(1, (3,))
            push(2, (3,))
            arrive(3, True)
            push(3, (1, 2))

        @pl.when(n == 2)
        def _():
            push(3, (3,))

        @pl.when(n == ROW_AT)
        def _():
            row_total()

        @pl.when(n == RECALL_AT)
        def _():
            recall()

        folds = jnp.where(chunk <= hi, 1, 0) + jnp.where(chunk <= lo, 1, 0)
        return early, jnp.minimum(ahead + jnp.where(n >= 2, folds, 0), N_SP)

    def take(chunk, n, ahead):
        keys = kv[chunk, 0:AD]
        d_hi, d_mid, d_lo = pieces(decay_of(chunk))
        extra = rows_of((d_hi, d_mid, d_lo, 1.0, 1.0, 1.0), 64, ROWS)
        kaug[:, 0:128] = jnp.concatenate([keys, extra.astype(bf16)], axis=0).T
        kaug[:, 128:256] = jnp.concatenate([keys, keys], axis=0).T

        def side(slot, _):
            mine = jnp.where(slot == 0, hi, lo)

            @pl.when(chunk < mine)
            def _():
                fold(slot, chunk, False)

            @pl.when(chunk == mine)
            def _():
                fold(slot, chunk, True)

            @pl.when((chunk <= mine) & (n >= 2) & (ahead + slot < N_SP))
            def _():
                arrive(ahead + slot, False)

            return 0

        lax.fori_loop(0, 2, side, 0)

    lax.fori_loop(0, 16, visit, (0, 4))

    depart(0)

    def o_wait(n, _):
        own = (n == head) & ((hi == r) | (lo == r))

        @pl.when(jnp.logical_not(own))
        def _():
            pltpu.make_async_remote_copy(
                ostage.at[0, 0], att.at[n], o_s.at[0, 0], o_r.at[n],
                device_id=(r, (t + 1) % N_TP), device_id_type=MESH,
            ).wait_recv()

        return 0

    def m_wait(n, _):
        @pl.when(n != t)
        def _():
            pltpu.make_async_remote_copy(
                mstage.at[0], mb.at[n], m_s.at[0], m_r.at[n],
                device_id=(r, (t + 1) % N_TP), device_id_type=MESH,
            ).wait_recv()

        return 0

    lax.fori_loop(0, N_TP, m_wait, 0)
    for copy in w_copies:
        copy.wait()

    m_all = jnp.concatenate([mb[n, 0:MD].astype(f32).T for n in range(N_TP)], axis=1)
    m_stats = sum(mb[n, MD:ZR].astype(f32) for n in range(N_TP)).T
    m_sq = m_stats[:, 0:1] + m_stats[:, 1:2] + m_stats[:, 2:3]
    m_mix = (m_all * lax.rsqrt(m_sq / 1024.0 + EPS) * mgain_in[...]).astype(bf16)

    for n in range(4):
        cols = slice(n * 512, n * 512 + 512)
        half[:, cols] = dot(m_mix, wm[:, cols])

    decay_copy().wait_send()
    for h in range(2):
        for own, copy in (q_copy(h), kv_copy(h)):

            @pl.when(jnp.logical_not(own))
            def _():
                copy.wait_send()

    for p in (1, 2, 3):
        wanted, copy = block_copy(p)

        @pl.when(wanted)
        def _():
            copy.wait_send()

    def z_done(to, _):
        @pl.when(to != ry)
        def _():
            z_copy(to).wait_send()

        return 0

    def row_done(to, _):
        row_copy(to).wait_send()
        return 0

    lax.fori_loop(0, 4, z_done, 0)
    lax.fori_loop(rz + 1, 4, row_done, 0)

    def f_done(n, _):
        chunk = chunk_at(n)
        mine = core_for(chunk) == b
        reaches = jnp.where(n < 4, True, chunk <= 15 - a)

        @pl.when(reaches & mine)
        def _():
            @pl.when((n > 0) & (n < 4))
            def _():
                for p in (1, 2, 3):
                    wanted, copy = peer_copy(chunk, n, p)

                    @pl.when(wanted)
                    def _():
                        copy.wait_send()

            @pl.when(sibling_uses(chunk))
            def _():
                forward_copy(chunk).wait_send()

        return 0

    lax.fori_loop(0, N_SP, f_done, 0)

    lax.fori_loop(0, 16, o_wait, 0)
    a_all = jnp.concatenate(
        [
            jnp.concatenate([att[2 * n], att[2 * n + 1]], axis=0).astype(f32).T
            for n in range(8)
        ],
        axis=1,
    )
    a_sq = jnp.sum(a_all * a_all, axis=1, keepdims=True)
    a_mix = (a_all * lax.rsqrt(a_sq / 1024.0 + EPS) * again_in[...]).astype(bf16)
    for n in range(4):
        cols = slice(n * 512, n * 512 + 512)
        out[:, cols] = (half[:, cols] + dot(a_mix, wa[:, cols])).astype(bf16)

    def p_done(p, _):
        for slot in range(2):
            own, copy = o_copy(slot, p)

            @pl.when(jnp.logical_not(own))
            def _():
                copy.wait_send()

        @pl.when(p != t)
        def _():
            m_copy(p).wait_send()

        return 0

    lax.fori_loop(0, N_TP, p_done, 0)


def mix(*arrays):
    smem = pl.BlockSpec(memory_space=pltpu.SMEM)
    hbm = pl.BlockSpec(memory_space=pltpu.HBM)
    dma = pltpu.SemaphoreType.DMA
    return pl.pallas_call(
        mix_kernel,
        out_shape=jax.ShapeDtypeStruct((128, 2048), bf16),
        in_specs=[smem] * 2 + [hbm] * 18,
        out_specs=pl.BlockSpec(memory_space=pltpu.VMEM),
        scratch_shapes=[
            pltpu.VMEM((ROWS, 2048), bf16),
            pltpu.VMEM((2048, 1024), bf16),
            pltpu.VMEM((8, 2048), bf16),
            pltpu.VMEM((1, 2048), f32),
            pltpu.VMEM((1, ROWS), f32),
            pltpu.VMEM((1, MD, MD), f32),
            pltpu.VMEM((1, MD), f32),
            pltpu.VMEM((1, 1024), f32),
            pltpu.VMEM((1, 1024), f32),
            pltpu.VMEM((2, AD, ROWS), bf16),
            pltpu.VMEM((2, 2 * AD, ROWS), bf16),
            pltpu.VMEM((MD, ROWS), bf16),
            pltpu.VMEM((ROWS, MD), bf16),
            pltpu.VMEM((MD, ROWS), bf16),
            pltpu.VMEM((8, ROWS), f32),
            pltpu.VMEM((8, ROWS), f32),
            pltpu.VMEM((ROWS, 8), f32),
            pltpu.VMEM((1024, 2048), bf16),
            pltpu.VMEM((1024, 2048), bf16),
            pltpu.VMEM((N_SP, 2 * AD + 16, ROWS), bf16),
            pltpu.VMEM((2, AD, ROWS), bf16),
            pltpu.VMEM((2, 2, N_SP * ROWS), f32),
            pltpu.VMEM((ROWS, 256), bf16),
            pltpu.VMEM((2, 256, ROWS), bf16),
            pltpu.VMEM((2, 8, ROWS), f32),
            pltpu.VMEM((2, VEXT, ROWS), f32),
            pltpu.VMEM((2, N_TP, AD, 128), bf16),
            pltpu.VMEM((16, AD, 128), bf16),
            pltpu.VMEM((ZR, MD), bf16),
            pltpu.VMEM((4, ZR, MD), bf16),
            pltpu.VMEM((ZR, MD), bf16),
            pltpu.VMEM((4, ZR, MD), bf16),
            pltpu.VMEM((N_TP, ZR, 128), bf16),
            pltpu.VMEM((N_TP, ZR, 128), bf16),
            pltpu.VMEM((ZR, ROWS), bf16),
            pltpu.VMEM((ZR, ROWS), f32),
            pltpu.VMEM((128, 2048), f32),
            dma((20,)), dma((8,)),
            dma((2,)), dma((N_SP,)),
            dma((2,)), dma((2,)),
            dma((4,)), dma((4,)), dma((4,)), dma((4,)),
            dma((N_TP,)), dma((N_TP,)),
            dma((2, N_TP)), dma((16,)),
            dma((4, 3)), dma((N_SP,)), dma, dma,
        ],
        compiler_params=pltpu.CompilerParams(
            collective_id=0, has_side_effects=True, vmem_limit_bytes=60 * 2**20
        ),
        cost_estimate=pl.CostEstimate(
            flops=60 * 10**9, bytes_accessed=12 * 2**20, transcendentals=0
        ),
    )(*arrays)


def on_device(tokens, norm_gain, attn_query, attn_key, attn_value, score_scale, attention_decay,
              mem_query, mem_key, mem_value, mem_ingate, input_shift, memory_decay, mem_outgate,
              init_memory, init_normalizer, attn_gain, mem_gain, attn_out, mem_out):
    return mix(
        score_scale, input_shift, tokens, attn_query, attn_key, attn_value, mem_query, mem_key,
        mem_value, mem_outgate, mem_ingate.T, norm_gain.reshape(1, 2048), memory_decay,
        attention_decay, init_memory, init_normalizer, attn_gain.reshape(1, 1024),
        mem_gain.reshape(1, 1024), attn_out, mem_out,
    )


def solution(mesh):
    tp = P(None, "tp")
    placed = (
        P("sp", None), P(), tp, tp, tp, P(), P("tp", None), tp, tp, tp, P(), P(),
        P("tp", "sp"), tp, P("tp", None, None), P("tp", None), P(), P(), P(), P(),
    )
    return jax.shard_map(
        on_device, mesh=mesh, in_specs=placed, out_specs=P(("sp", "tp"), None), check_vma=False
    )
```
